128 devices in a mesh: sp: 32 (over z, y, core), tp: 4 (over x).
Axes of the slice: x: 4, y: 4, z: 4, core: 2. Of those that a mesh axis runs over, the one named last changes fastest.
Arguments:
- queries: bfloat16 [16384, 2048], P('sp', 'tp'), may hold values from -6 to 6
- keys: bfloat16 [16384, 512], P('sp', 'tp'), may hold values from -6 to 6
- values: bfloat16 [16384, 512], P('sp', 'tp'), may hold values from -6 to 6
- residual: bfloat16 [16384, 2048], P(('sp', 'tp')), may hold values from -0.119628906 to 0.119628906
- out_proj: bfloat16 [2048, 2048], replicated, may hold values from -0.125 to 0.125
- query_gain: float32 [128], replicated, may hold values from 0.7 to 7
- key_gain: float32 [128], replicated, may hold values from 0.7 to 7
- norm_gain: float32 [2048], replicated, may hold values from 0.1 to 1.9
- routes: int32 [16384, 4], P(('sp', 'tp')), may hold values from 0 to 127, all different within a row; in each aligned block of 128 rows (0 to 127, 128 to 255, ...) at most 8 rows name the same one
- route_weight: float32 [16384, 4], P(('sp', 'tp')), may hold values from 0.1 to 1
- expert_gate: bfloat16 [128, 2048, 256], P(('sp', 'tp')), may hold values from -0.125 to 0.125
- expert_up: bfloat16 [128, 2048, 256], P(('sp', 'tp')), may hold values from -0.125 to 0.125
- expert_down: bfloat16 [128, 256, 2048], P(('sp', 'tp')), may hold values from -0.375 to 0.375
- shared_gate: bfloat16 [2048, 256], replicated, may hold values from -0.125 to 0.125
- shared_up: bfloat16 [2048, 256], replicated, may hold values from -0.125 to 0.125
- shared_down: bfloat16 [256, 2048], replicated, may hold values from -0.375 to 0.375
Outputs:
- layer_out: bfloat16 [16384, 2048], P(('sp', 'tp'))
The draws below stay inside these ranges and needn't reach their ends.
Inputs may be any that keep to these rules, and one draw needn't show every extreme that they name: In the rows of one device (aligned blocks of 128 tokens), no expert is named by more than 8 routes; some expert is named by exactly 8 routes of some device; the 4 experts of a token differ.
All inputs are finite; a program needn't handle non-finite values.
Results may differ from the reference program's by a relative error of at most 0.023.
The reference program's roundings to bfloat16 on the way count: a program that leaves them out, or rounds other values in their place, can miss the bound.
Values may be sent and summed in bfloat16 or wider, within the bound.
A program may use at most 128 MiB of HBM per device.

```python
import math
import jax
import jax.numpy as jnp
import numpy as np
from jax import lax

D = 2048
HEADS = 16
KV_HEADS = 4
HD = 128
EFF = 256
SFF = 256
GRID_W = 64
TOP = 4
SEQ = 16384
ROWS_DEV = 128
EXPERTS = 128
CAP = 8
N_SP = 32
N_TP = 4


def paired_draw(key):
    key_rows = jax.random.normal(jax.random.fold_in(key, 11), (SEQ, KV_HEADS * HD), jnp.float32)
    query_rows = jax.random.normal(jax.random.fold_in(key, 12), (SEQ, HEADS * HD), jnp.float32)
    return (jnp.clip(query_rows, -6.0, 6.0), jnp.clip(key_rows, -6.0, 6.0))


def draw_queries(key, part):
    return paired_draw(key)[0].astype(jnp.bfloat16)


def draw_keys(key, part):
    return paired_draw(key)[1].astype(jnp.bfloat16)


def gain_draw(key):
    return jax.random.uniform(key, (HD,), jnp.float32, 0.7, 1.3)


def draw_query_gain(key, part):
    return gain_draw(jax.random.fold_in(key, 21))


def draw_key_gain(key, part):
    return gain_draw(jax.random.fold_in(key, 22))


def block_scale(rng, shape, cuts, low, largest):
    def one(dim, blocks):
        heights = jax.random.uniform(jax.random.fold_in(jax.random.fold_in(rng, 6), dim), (blocks,), jnp.float32, low / len(cuts), largest / len(cuts))
        return jnp.repeat(jnp.exp(heights), shape[dim] // blocks).reshape((-1,) + (1,) * (len(shape) - dim - 1))

    loudness = one(*cuts[0])
    for cut in cuts[1:]:
        loudness = loudness * one(*cut)
    return loudness


def deal_out(own_key, own, number, rows, amount, top, limit, slope):
    ranking = jax.random.permutation(own_key, amount)
    heavy_load, common = portions_of(amount, rows * top, limit, slope, True), portions_of(amount, rows * top, limit, slope, False)
    places = jnp.arange(amount)

    def named(sizes, rotation):
        used = int((sizes > 0).sum())
        fixed = max(1, used // 4)
        passed = fixed + (places - fixed + rotation * (used - fixed)) % max(1, amount - fixed)
        return jnp.zeros((amount,), jnp.int32).at[ranking[jnp.where(places < fixed, places, passed)]].set(jnp.asarray(sizes, jnp.int32))

    sizes = jnp.where(number % 4 == 0, named(heavy_load, number // 4), named(common, number - number // 4 - 1))
    mixed = jax.random.permutation(jax.random.fold_in(own, 3), amount)
    source_of, taker = mixed[0:amount // 2 * 2:2], mixed[1:amount // 2 * 2:2]
    margin = jnp.minimum(sizes[source_of] - 1, limit - sizes[taker]) // 2
    margin = jnp.where((source_of == ranking[0]) | (taker == ranking[0]) | (sizes[taker] == 0), 0, jnp.maximum(margin, 0))
    passed = jax.random.randint(jax.random.fold_in(own, 4), (amount // 2,), 0, 1 << 20) % (margin + 1)
    sizes = sizes.at[source_of].add(-passed).at[taker].add(passed)
    members = jnp.searchsorted(jnp.cumsum(sizes), jnp.arange(rows * top), side="right").astype(jnp.int32)
    listing = members.reshape(top, rows).T
    listing = listing[jax.random.permutation(jax.random.fold_in(own, 1), rows)]
    rotation = jax.random.randint(jax.random.fold_in(own, 2), (rows, 1), 0, top)
    return jnp.take_along_axis(listing, (jnp.arange(top)[None, :] + rotation) % top, axis=1)


def portions_of(count, total, limit, lean, full):
    portions = [(1 << 20) // math.isqrt(standing ** lean) + 1 for standing in range(1, count + 1)]
    largest = limit if full else min(limit, max(-(-total // count), total * portions[0] // sum(portions)))
    least = 1 if total - largest >= count - 1 else 0
    given, rest = [largest] + [least] * (count - 1), total - largest - least * (count - 1)
    while rest > 0:
        movable = [i for i in range(1, count) if given[i] < largest] or [i for i in range(1, count) if given[i] < limit]
        pool, remaining = sum([portions[i] for i in movable]), rest
        for i in movable:
            extra = min(limit - given[i], max(1, remaining * portions[i] // pool), rest)
            given[i] = given[i] + extra
            rest = rest - extra
    return np.array(given)


def gaussian(key, shape, spread, reach, cuts=(), kind=jnp.bfloat16):
    loudness = block_scale(key, shape, cuts, -0.22, 0.18) if cuts else 1.0
    values = jax.random.normal(key, shape, jnp.float32) * spread * loudness
    return jnp.minimum(jnp.maximum(values, -reach), reach).astype(kind)


def setup_inputs(seed: int = 0) -> dict:
    key_of = jax.random.split(jax.random.key(seed), 17)
    queries = draw_queries(jax.random.fold_in(key_of[16], 71), 0)
    keys = draw_keys(jax.random.fold_in(key_of[16], 71), 0)
    values = gaussian(key_of[2], (SEQ, KV_HEADS * HD), 1.0, 6.0, ((0, 32), (1, 4)))
    residual = gaussian(key_of[3], (SEQ, D), 0.02, 0.119628906, ((0, 128),))
    out_proj = gaussian(key_of[4], (HEADS * HD, D), (HEADS * HD) ** -0.5, 0.125)
    query_gain = draw_query_gain(jax.random.fold_in(key_of[16], 71), 0)
    key_gain = draw_key_gain(jax.random.fold_in(key_of[16], 71), 0)
    norm_gain = jnp.clip(1.0 + 0.18 * jax.random.normal(key_of[7], (D,), jnp.float32), 0.1, 1.9)
    routes_keys = jax.random.split(jax.random.fold_in(key_of[8], 1), SEQ // ROWS_DEV)
    routes_turns = jax.random.permutation(jax.random.fold_in(key_of[8], 3), SEQ // ROWS_DEV)
    routes = jax.vmap(lambda own, number: deal_out(jax.random.fold_in(key_of[8], 2), own, number, ROWS_DEV, EXPERTS, TOP, CAP, 2))(routes_keys, routes_turns).reshape((SEQ, TOP))
    route_weight = jnp.clip(jnp.exp(math.log(1.0) - 2.3025851 * jax.random.uniform(key_of[9], (SEQ, TOP), jnp.float32) ** block_scale(key_of[9], (SEQ, TOP), ((0, 128),), -0.2, 0.2)), 0.1, 1.0)
    expert_gate = gaussian(key_of[10], (EXPERTS, D, EFF), D ** -0.5, 0.125, ((0, 128),))
    expert_up = gaussian(key_of[11], (EXPERTS, D, EFF), D ** -0.5, 0.125, ((0, 128),))
    expert_down = gaussian(key_of[12], (EXPERTS, EFF, D), EFF ** -0.5, 0.375, ((0, 128),))
    shared_gate = gaussian(key_of[13], (D, SFF), D ** -0.5, 0.125)
    shared_up = gaussian(key_of[14], (D, SFF), D ** -0.5, 0.125)
    shared_down = gaussian(key_of[15], (SFF, D), SFF ** -0.5, 0.375)
    return dict(queries=queries, keys=keys, values=values, residual=residual, out_proj=out_proj, query_gain=query_gain, key_gain=key_gain, norm_gain=norm_gain, routes=routes, route_weight=route_weight, expert_gate=expert_gate, expert_up=expert_up, expert_down=expert_down, shared_gate=shared_gate, shared_up=shared_up, shared_down=shared_down)


EPS = 1e-06
THETA = 10000.0

def rotate_pairs(block, cosine, sine):
    first, second = jnp.split(block, 2, axis=-1)
    return jnp.concatenate([first * cosine - second * sine, second * cosine + first * sine], axis=-1)

def normed_rotary(source, gain, heads, offset):
    count = source.shape[0]
    width = gain.shape[0]
    values_f = source.astype(jnp.float32).reshape(count, heads, width)
    values_f = values_f * lax.rsqrt(lax.optimization_barrier(jnp.mean(values_f * values_f, axis=-1, keepdims=True)) + EPS) * gain
    position = offset + jnp.arange(count, dtype=jnp.int32)
    grid_row = (position // GRID_W).astype(jnp.float32)
    grid_col = (position % GRID_W).astype(jnp.float32)
    quarter = width // 4
    inverse = jnp.power(THETA, -4.0 * jnp.arange(quarter, dtype=jnp.float32) / width)
    row_angle = (grid_row[:, None] * inverse[None, :])[:, None, :]
    col_angle = (grid_col[:, None] * inverse[None, :])[:, None, :]
    row_half, col_half = jnp.split(values_f, 2, axis=-1)
    turned = jnp.concatenate([rotate_pairs(row_half, jnp.cos(row_angle), jnp.sin(row_angle)), rotate_pairs(col_half, jnp.cos(col_angle), jnp.sin(col_angle))], axis=-1)
    return turned.reshape(count, heads * width).astype(jnp.bfloat16)

def reference(queries, keys, values, residual, out_proj, query_gain, key_gain, norm_gain, routes, route_weight, expert_gate, expert_up, expert_down, shared_gate, shared_up, shared_down):
    tokens = queries.shape[0]
    width = query_gain.shape[0]
    group = HEADS // KV_HEADS
    scale = 1.0 / math.sqrt(width)
    q_rot = normed_rotary(queries, query_gain, HEADS, 0)
    k_rot = normed_rotary(keys, key_gain, KV_HEADS, 0)
    key_f = k_rot.reshape(tokens, KV_HEADS, width).astype(jnp.float32).transpose(1, 0, 2)
    value_f = values.reshape(tokens, KV_HEADS, width).astype(jnp.float32).transpose(1, 0, 2)
    block = math.gcd(tokens, 512)
    q_blocks = q_rot.reshape(tokens // block, block, KV_HEADS, group, width).transpose(0, 2, 3, 1, 4)

    def attend_head(operands):
        query_part, key_part, value_part = operands
        scores = jnp.einsum('gqd,kd->gqk', query_part.astype(jnp.float32), key_part) * scale
        top = lax.optimization_barrier(jnp.max(scores, axis=-1, keepdims=True))
        weights = jnp.exp(scores - top)
        denom = lax.optimization_barrier(jnp.sum(weights, axis=-1, keepdims=True))
        rounded = weights.astype(jnp.bfloat16).astype(jnp.float32)
        summed = jnp.einsum('gqk,kd->gqd', rounded, value_part)
        return (summed / denom).astype(jnp.bfloat16)

    def attend_block(query_block):
        return lax.map(attend_head, (query_block, key_f, value_f))
    outputs = lax.map(attend_block, q_blocks)
    attn_heads = outputs.transpose(0, 3, 1, 2, 4).reshape(tokens, HEADS * width)
    projected = jnp.dot(attn_heads, out_proj, preferred_element_type=jnp.float32)
    hidden1 = (residual.astype(jnp.float32) + projected).astype(jnp.bfloat16)
    hidden_f = hidden1.astype(jnp.float32)
    normed = (hidden_f * lax.rsqrt(lax.optimization_barrier(jnp.mean(hidden_f * hidden_f, axis=-1, keepdims=True)) + EPS) * norm_gain).astype(jnp.bfloat16)
    shared_hidden = (jax.nn.silu(jnp.dot(normed, shared_gate, preferred_element_type=jnp.float32)) * jnp.dot(normed, shared_up, preferred_element_type=jnp.float32)).astype(jnp.bfloat16)
    shared_out = jnp.dot(shared_hidden, shared_down, preferred_element_type=jnp.float32)
    pairs = tokens * TOP
    flat_routes = routes.reshape(pairs)
    bound = N_SP * N_TP * CAP
    padded = jnp.concatenate([normed, jnp.zeros((1, normed.shape[1]), jnp.bfloat16)], axis=0)

    def one_expert(expert, buffer):
        picked = jnp.nonzero(flat_routes == expert, size=bound, fill_value=pairs)[0].astype(jnp.int32)
        rows = padded[picked // TOP]
        hidden_e = (jax.nn.silu(jnp.dot(rows, expert_gate[expert], preferred_element_type=jnp.float32)) * jnp.dot(rows, expert_up[expert], preferred_element_type=jnp.float32)).astype(jnp.bfloat16)
        result = jnp.dot(hidden_e, expert_down[expert], preferred_element_type=jnp.float32).astype(jnp.bfloat16)
        return buffer.at[picked].set(result)
    buffer = lax.fori_loop(0, EXPERTS, one_expert, jnp.zeros((pairs + 1, normed.shape[1]), jnp.bfloat16))
    routed = buffer[:pairs].reshape(tokens, TOP, normed.shape[1]).astype(jnp.float32)
    mixed = jnp.einsum('tk,tkd->td', route_weight, routed) + shared_out
    return (hidden_f + mixed).astype(jnp.bfloat16)
```

```python
import functools
import math

import jax
import jax.numpy as jnp
import numpy as np
from jax import lax
from jax.experimental import pallas as pl
from jax.experimental.pallas import tpu as pltpu
from jax.sharding import PartitionSpec as P

HEADS = 16
KV_HEADS = 4
GRID_W = 64
HD = 128
TOK = 512
EPS = 1e-06
THETA = 10000.0
MESH = pl.DeviceIdType.MESH
F32 = jnp.float32
BF16 = jnp.bfloat16


def rotary_tables():
    quarter = HD // 4
    inverse = (THETA ** (-4.0 * np.arange(quarter, dtype=np.float64) / HD)).astype(np.float32)

    def table(count):
        angle = np.arange(count, dtype=np.float32)[:, None] * inverse[None, :]
        angle = angle.astype(np.float32).astype(np.float64)
        cosine = np.cos(angle).astype(np.float32)
        sine = np.sin(angle).astype(np.float32)
        return np.concatenate([cosine, cosine], 1), np.concatenate([-sine, sine], 1)

    row_cos, row_sin = table(256)
    col_cos, col_sin = table(GRID_W)
    zr, zc = np.zeros_like(row_cos), np.zeros_like(col_cos)
    rows = np.stack([np.concatenate([row_cos, zr], 1), np.concatenate([row_sin, zr], 1)])
    cols = np.stack([np.concatenate([zc, col_cos], 1), np.concatenate([zc, col_sin], 1)])
    return rows, cols


def normed_rotary(source, gain, cos_t, sin_t):
    x = source.astype(F32)
    x = x * lax.rsqrt(jnp.mean(x * x, axis=-1, keepdims=True) + EPS) * gain
    lane = lax.broadcasted_iota(jnp.int32, x.shape, 1)
    partner = jnp.where((lane // 32) % 2 == 0, pltpu.roll(x, 96, 1), pltpu.roll(x, 32, 1))
    return x * cos_t + partner * sin_t


A_SET = ((1, 0), (3, 0), (0, 1), (0, 3))
B_SET = ((1, 1), (1, 3), (3, 1), (3, 3))
C_SET = ((2, 0), (0, 2))
D_SET = ((2, 1), (2, 3), (1, 2), (3, 2))
E_SET = ((2, 2),)


def attention_kernel(
    q_ref,
    k_ref,
    v_ref,
    qg_ref,
    kg_ref,
    rows_ref,
    cols_ref,
    hx_ref,
    kt_all,
    v_all,
    q_hl,
    trig,
    acc,
    mstate,
    o_tok,
    send_sem,
    krecv,
    vrecv,
    xrecv,
):
    sp = lax.axis_index("sp")
    tx = lax.axis_index("tp")
    core = sp % 2
    yy = (sp // 2) % 4
    zz = sp // 8

    def at(y, z, c):
        return (z % 4) * 8 + (y % 4) * 2 + c

    sib = at(yy, zz, 1 - core)
    y_next, y_prev = at(yy + 1, zz, core), at(yy + 3, zz, core)
    z_next, z_prev = at(yy, zz + 1, core), at(yy, zz + 3, core)

    barrier = pltpu.get_barrier_semaphore()
    for peer in (sib, y_next, y_prev, z_next, z_prev):
        pl.semaphore_signal(barrier, inc=1, device_id=(peer, tx), device_id_type=MESH)
    for step in (1, 2, 3):
        pl.semaphore_signal(
            barrier, inc=1, device_id=(sp, (tx + step) % 4), device_id_type=MESH
        )

    counter = [0]
    sent = []

    def push(kind, slot, peer):
        buf, recv = (kt_all, krecv) if kind == 0 else (v_all, vrecv)
        copy = pltpu.make_async_remote_copy(
            src_ref=buf.at[slot],
            dst_ref=buf.at[slot],
            send_sem=send_sem.at[counter[0]],
            recv_sem=recv.at[slot],
            device_id=(peer, tx),
            device_id_type=MESH,
        )
        sent.append((kind, counter[0]))
        counter[0] += 1
        copy.start()

    def arrived(kind, slot):
        buf, recv = (kt_all, krecv) if kind == 0 else (v_all, vrecv)
        pltpu.make_async_remote_copy(
            src_ref=buf.at[slot],
            dst_ref=buf.at[slot],
            send_sem=send_sem.at[0],
            recv_sem=recv.at[slot],
            device_id=(sib, tx),
            device_id_type=MESH,
        ).wait_recv()

    def origin(dy, dz, c):
        return at(yy - dy + 4, zz - dz + 4, c)

    for r in range(8):
        sl = pl.ds(r * GRID_W, GRID_W)
        for i in range(2):
            trig[i, sl, :] = rows_ref[i, pl.ds(sp * 8 + r, 1), :] + cols_ref[i]

    kr = normed_rotary(k_ref[...], kg_ref[...], trig[0], trig[1])
    kt_all[sp] = kr.T.astype(BF16)
    v_all[sp] = v_ref[...]
    pl.semaphore_wait(barrier, 8)
    for kind in (0, 1):
        for peer in (y_next, y_prev, z_next, z_prev):
            push(kind, sp, peer)
    push(0, sp, sib)
    push(1, sp, sib)

    factor = math.log2(math.e) / math.sqrt(HD)
    for h in range(4):
        qr = normed_rotary(q_ref[:, h * HD : (h + 1) * HD], qg_ref[...], trig[0], trig[1])
        qs = qr.astype(BF16).astype(F32) * factor
        hi = qs.astype(BF16)
        q_hl[h * TOK : (h + 1) * TOK, 0:HD] = hi
        q_hl[h * TOK : (h + 1) * TOK, HD : 2 * HD] = (qs - hi.astype(F32)).astype(BF16)
    acc[...] = jnp.zeros_like(acc)
    mstate[...] = jnp.full_like(mstate, -1e30)

    def attend(slots):
        n = len(slots)
        width = n * TOK
        kt = jnp.concatenate([kt_all[s] for s in slots], axis=1)
        k2 = jnp.concatenate([kt, kt], axis=0)
        vv = jnp.concatenate([v_all[s] for s in slots], axis=0)
        v2 = jnp.concatenate([vv, jnp.ones_like(vv)], axis=1)

        def scores(h):
            return jnp.dot(
                q_hl[h * TOK : (h + 1) * TOK, :], k2, preferred_element_type=F32
            )

        s = scores(0)
        for h in range(4):
            sl = slice(h * TOK, (h + 1) * TOK)
            old = mstate[sl, :]
            top = s[:, 0:HD]
            for j in range(1, width // HD):
                top = jnp.maximum(top, s[:, j * HD : (j + 1) * HD])
            new = jnp.maximum(old, jnp.max(top, axis=1, keepdims=True))
            mstate[sl, :] = new
            p = jnp.exp2(s - new[:, 0:1]).astype(BF16)
            if h < 3:
                s = scores(h + 1)
            shrink = jnp.exp2(old - new)
            pv = jnp.dot(p, v2, preferred_element_type=F32)
            acc[sl, :] = acc[sl, :] * jnp.concatenate([shrink, shrink], axis=1) + pv

    def pair_arrived(dy, dz, c):
        slot = origin(dy, dz, c)
        arrived(0, slot)
        arrived(1, slot)

    def to_sibling(group):
        for dy, dz in group:
            slot = origin(dy, dz, core)
            push(0, slot, sib)
            push(1, slot, sib)

    arrived(0, sib)
    arrived(1, sib)
    attend([sp, sib])

    def event(t):
        if t == 0:
            for dy, dz in A_SET:
                pair_arrived(dy, dz, core)
            turn = 1 + 2 * core
            for d in (1, 3):
                push(0, origin(d, 0, core), z_next)
                push(0, origin(d, 0, core), z_prev)
                push(1, origin(0, d, core), y_next)
                push(1, origin(0, d, core), y_prev)
            push(0, origin(turn, 0, core), at(yy + turn, zz, core))
            push(1, origin(0, turn, core), at(yy, zz + turn, core))
            push(0, origin(0, 1, core), z_next)
            push(1, origin(1, 0, core), y_next)
            to_sibling(A_SET)
        if t == 1:
            for dy, dz in A_SET:
                pair_arrived(dy, dz, 1 - core)
        if t == 2:
            for dy, dz in B_SET + C_SET:
                pair_arrived(dy, dz, core)
            push(0, origin(2, 0, core), z_next)
            push(0, origin(2, 0, core), z_prev)
            push(1, origin(0, 2, core), y_next)
            push(1, origin(0, 2, core), y_prev)
            push(0, origin(1, 1, core), z_next)
            push(0, origin(3, 3, core), z_prev)
            push(1, origin(1, 1, core), y_next)
            push(1, origin(3, 3, core), y_prev)
            to_sibling(B_SET + C_SET)
        if t == 3:
            for dy, dz in B_SET:
                pair_arrived(dy, dz, 1 - core)
        if t == 4:
            for dy, dz in D_SET:
                pair_arrived(dy, dz, core)
            push(0, origin(2, 3, core), z_prev)
            push(1, origin(3, 2, core), y_prev)
            to_sibling(D_SET)
            for dy, dz in C_SET:
                pair_arrived(dy, dz, 1 - core)
        if t == 5:
            pair_arrived(2, 2, core)
            to_sibling(E_SET)
        if t == 6:
            for dy, dz in D_SET:
                pair_arrived(dy, dz, 1 - core)

    groups = (
        [(dy, dz, 0) for dy, dz in A_SET],
        [(dy, dz, 1) for dy, dz in A_SET],
        [(dy, dz, 0) for dy, dz in B_SET],
        [(dy, dz, 1) for dy, dz in B_SET],
        [(2, 0, 0), (0, 2, 0), (2, 0, 1), (0, 2, 1)],
        [(dy, dz, 0) for dy, dz in D_SET],
        [(dy, dz, 1) for dy, dz in D_SET],
    )

    def chosen(values, t):
        code = sum(v * 4**i for i, v in enumerate(values))
        out = (code >> (2 * t)) % 4
        return out

    def one_step(t, carry):
        for i in range(7):

            @pl.when(t == i)
            def _(i=i):
                event(i)

        slots = []
        for j in range(4):
            dy = chosen([g[j][0] for g in groups], t)
            dz = chosen([g[j][1] for g in groups], t)
            flip = chosen([g[j][2] for g in groups], t)
            slots.append(origin(dy, dz, (core + flip) % 2))
        attend(slots)
        return carry

    lax.fori_loop(0, 7, one_step, 0)
    pair_arrived(2, 2, 1 - core)
    attend([origin(2, 2, core), origin(2, 2, 1 - core)])

    for h in range(4):
        sl = slice(h * TOK, (h + 1) * TOK)
        o = (acc[sl, 0:HD] / acc[sl, HD : 2 * HD]).astype(BF16)
        for j in range(4):
            o_tok[j, :, h * HD : (h + 1) * HD] = o[j * 128 : (j + 1) * 128, :]
    exchanges = []
    for step in (1, 2, 3):
        peer = (tx + step) % 4
        copy = pltpu.make_async_remote_copy(
            src_ref=o_tok.at[peer],
            dst_ref=hx_ref.at[tx],
            send_sem=send_sem.at[counter[0]],
            recv_sem=xrecv.at[tx],
            device_id=(sp, peer),
            device_id_type=MESH,
        )
        counter[0] += 1
        copy.start()
        exchanges.append(copy)
    hx_ref[tx] = o_tok[tx]
    for step in (1, 2, 3):
        source = (tx + step) % 4
        pltpu.make_async_remote_copy(
            src_ref=o_tok.at[source],
            dst_ref=hx_ref.at[source],
            send_sem=send_sem.at[0],
            recv_sem=xrecv.at[source],
            device_id=(sp, source),
            device_id_type=MESH,
        ).wait_recv()
    for copy in exchanges:
        copy.wait_send()
    for kind, index in sent:
        buf, recv = (kt_all, krecv) if kind == 0 else (v_all, vrecv)
        pltpu.make_async_remote_copy(
            src_ref=buf.at[sp],
            dst_ref=buf.at[sp],
            send_sem=send_sem.at[index],
            recv_sem=recv.at[sp],
            device_id=(sib, tx),
            device_id_type=MESH,
        ).wait_send()


def attention(queries, keys, values, query_gain, key_gain):
    rows, cols = rotary_tables()
    vmem = pl.BlockSpec(memory_space=pltpu.VMEM)
    return pl.pallas_call(
        attention_kernel,
        out_shape=jax.ShapeDtypeStruct((4, 128, 512), BF16),
        in_specs=[vmem] * 7,
        out_specs=vmem,
        scratch_shapes=[
            pltpu.VMEM((32, HD, TOK), BF16),
            pltpu.VMEM((32, TOK, HD), BF16),
            pltpu.VMEM((4 * TOK, 2 * HD), BF16),
            pltpu.VMEM((2, TOK, HD), F32),
            pltpu.VMEM((4 * TOK, 2 * HD), F32),
            pltpu.VMEM((4 * TOK, HD), F32),
            pltpu.VMEM((4, 128, 4 * HD), BF16),
            pltpu.SemaphoreType.DMA((72,)),
            pltpu.SemaphoreType.DMA((32,)),
            pltpu.SemaphoreType.DMA((32,)),
            pltpu.SemaphoreType.DMA((4,)),
        ],
        compiler_params=pltpu.CompilerParams(
            collective_id=0, has_side_effects=True, vmem_limit_bytes=56 * 2**20
        ),
        name="attention",
    )(
        queries,
        keys,
        values,
        query_gain.reshape(1, HD),
        key_gain.reshape(1, HD),
        jnp.asarray(rows),
        jnp.asarray(cols),
    )


def expert_apply(arrived, expert_gate, expert_up, expert_down):
    sources, slots, width = arrived.shape
    local = expert_gate.shape[0]
    grouped = arrived.reshape(sources // local, local, slots, width)
    gate_part = jnp.einsum("sech,ehf->secf", grouped, expert_gate, preferred_element_type=F32)
    up_part = jnp.einsum("sech,ehf->secf", grouped, expert_up, preferred_element_type=F32)
    hidden_e = (jax.nn.silu(gate_part) * up_part).astype(BF16)
    result = jnp.einsum("secf,efh->sech", hidden_e, expert_down, preferred_element_type=F32)
    return result.astype(BF16).reshape(sources, slots, width)


def body(
    queries,
    keys,
    values,
    residual,
    out_proj,
    query_gain,
    key_gain,
    norm_gain,
    routes,
    route_weight,
    expert_gate,
    expert_up,
    expert_down,
    shared_gate,
    shared_up,
    shared_down,
):
    heads_x = attention(queries, keys, values, query_gain, key_gain)
    all_heads = heads_x.transpose(1, 0, 2).reshape(128, 2048)
    projected = jnp.dot(all_heads, out_proj, preferred_element_type=F32)
    hidden1 = (residual.astype(F32) + projected).astype(BF16)
    hidden_f = hidden1.astype(F32)
    normed = (
        hidden_f
        * lax.rsqrt(jnp.mean(hidden_f * hidden_f, axis=-1, keepdims=True) + EPS)
        * norm_gain
    ).astype(BF16)
    rows_local = normed.shape[0]
    top_count = routes.shape[1]
    pair_count = rows_local * top_count
    expert_total = expert_gate.shape[0] * lax.axis_size("sp") * lax.axis_size("tp")
    capacity = 8
    flat_routes = routes.reshape(pair_count)
    one_hot = (flat_routes[:, None] == jnp.arange(expert_total, dtype=jnp.int32)[None, :]).astype(
        F32
    )
    lower = (jnp.arange(pair_count)[:, None] >= jnp.arange(pair_count)[None, :]).astype(F32)
    running_count = jnp.dot(lower, one_hot, precision=lax.Precision.HIGHEST)
    slot_place = (jnp.sum(running_count * one_hot, axis=1) - 1.0).astype(jnp.int32)
    slot_index = flat_routes * capacity + slot_place
    slot_total = expert_total * capacity
    placement = (jnp.arange(slot_total, dtype=jnp.int32)[:, None] == slot_index[None, :]).astype(
        BF16
    )
    placement = jnp.sum(placement.reshape(slot_total, rows_local, top_count), axis=2)
    send_rows = jnp.dot(placement, normed, preferred_element_type=F32).astype(BF16)
    send_rows = send_rows.reshape(expert_total, capacity, normed.shape[1])
    shared_hidden = (
        jax.nn.silu(jnp.dot(normed, shared_gate, preferred_element_type=F32))
        * jnp.dot(normed, shared_up, preferred_element_type=F32)
    ).astype(BF16)
    shared_out = jnp.dot(shared_hidden, shared_down, preferred_element_type=F32)
    processed = expert_apply(
        lax.all_to_all(send_rows, ("sp", "tp"), split_axis=0, concat_axis=0, tiled=True),
        expert_gate,
        expert_up,
        expert_down,
    )
    returned = lax.all_to_all(processed, ("sp", "tp"), split_axis=0, concat_axis=0, tiled=True)
    returned = returned.reshape(slot_total, normed.shape[1])
    routed = returned[slot_index].reshape(rows_local, top_count, normed.shape[1]).astype(F32)
    mixed = jnp.einsum("tk,tkd->td", route_weight, routed) + shared_out
    return (hidden_f + mixed).astype(BF16)


def solution(mesh):
    placed = (
        P("sp", "tp"),
        P("sp", "tp"),
        P("sp", "tp"),
        P(("sp", "tp"), None),
        P(),
        P(),
        P(),
        P(),
        P(("sp", "tp"), None),
        P(("sp", "tp"), None),
        P(("sp", "tp"), None, None),
        P(("sp", "tp"), None, None),
        P(("sp", "tp"), None, None),
        P(),
        P(),
        P(),
    )
    return jax.shard_map(
        body, mesh=mesh, in_specs=placed, out_specs=P(("sp", "tp"), None), check_vma=False
    )
```

```python
import math

import jax
import jax.numpy as jnp
import numpy as np
from jax import lax
from jax.experimental import pallas as pl
from jax.experimental.pallas import tpu as pltpu
from jax.sharding import PartitionSpec as P

HEADS = 16
KV_HEADS = 4
GRID_W = 64
HD = 128
TOK = 512
EPS = 1e-06
THETA = 10000.0
MESH = pl.DeviceIdType.MESH
F32 = jnp.float32
BF16 = jnp.bfloat16


def rotary_tables():
    quarter = HD // 4
    inverse = (THETA ** (-4.0 * np.arange(quarter, dtype=np.float64) / HD)).astype(np.float32)

    def table(count):
        angle = np.arange(count, dtype=np.float32)[:, None] * inverse[None, :]
        angle = angle.astype(np.float32).astype(np.float64)
        cosine = np.cos(angle).astype(np.float32)
        sine = np.sin(angle).astype(np.float32)
        return np.concatenate([cosine, cosine], 1), np.concatenate([-sine, sine], 1)

    row_cos, row_sin = table(256)
    col_cos, col_sin = table(GRID_W)
    zr, zc = np.zeros_like(row_cos), np.zeros_like(col_cos)
    rows = np.stack([np.concatenate([row_cos, zr], 1), np.concatenate([row_sin, zr], 1)])
    cols = np.stack([np.concatenate([zc, col_cos], 1), np.concatenate([zc, col_sin], 1)])
    return rows, cols


def normed_rotary(source, gain, cos_t, sin_t):
    x = source.astype(F32)
    x = x * lax.rsqrt(jnp.mean(x * x, axis=-1, keepdims=True) + EPS) * gain
    lane = lax.broadcasted_iota(jnp.int32, x.shape, 1)
    partner = jnp.where((lane // 32) % 2 == 0, pltpu.roll(x, 96, 1), pltpu.roll(x, 32, 1))
    return x * cos_t + partner * sin_t


A_SET = ((1, 0), (3, 0), (0, 1), (0, 3))
B_SET = ((1, 1), (1, 3), (3, 1), (3, 3))
C_SET = ((2, 0), (0, 2))
D_SET = ((2, 1), (2, 3), (1, 2), (3, 2))
E_SET = ((2, 2),)


COLS = ((0, 640), (640, 1280), (1280, 2048))


def layer_kernel(
    q_ref,
    k_ref,
    v_ref,
    qg_ref,
    kg_ref,
    rows_ref,
    cols_ref,
    ng_ref,
    routes_ref,
    rweight_ref,
    residual_hbm,
    out_proj_hbm,
    gate_hbm,
    up_hbm,
    down_hbm,
    sgate_hbm,
    sup_hbm,
    sdown_hbm,
    out_ref,
    hx_ref,
    kt_all,
    v_all,
    q_hl,
    trig,
    acc,
    mstate,
    o_tok,
    residual,
    gate,
    up,
    down,
    sgate,
    sup,
    sdown,
    hidden,
    shared,
    meta,
    place,
    mixw,
    nbx,
    nby,
    nbz,
    sendx,
    sendy,
    sendz,
    gotx,
    goty,
    gotz,
    backx,
    backy,
    backz,
    finx,
    finy,
    finz,
    gsum,
    hsum,
    send_sem,
    krecv,
    vrecv,
    xrecv,
    load_sem,
    ring_send,
    ring_recv,
    plane_send,
    plane_recv,
):
    near = (nbx, nby, nbz)
    sending = (sendx, sendy, sendz)
    got = (gotx, goty, gotz)
    back = (backx, backy, backz)
    fin = (finx, finy, finz)
    loads = [
        pltpu.make_async_copy(src, dst, load_sem.at[i])
        for i, (src, dst) in enumerate(
            (
                (residual_hbm, residual),
                (gate_hbm.at[0], gate),
                (up_hbm.at[0], up),
                (down_hbm.at[0], down),
                (sgate_hbm, sgate),
                (sup_hbm, sup),
                (sdown_hbm, sdown),
            )
        )
    ]
    for d, (lo, hi) in enumerate(COLS):
        for half, dst in enumerate((back[d], sending[d])):
            src = out_proj_hbm.at[pl.ds(half * 32, 32), :, lo:hi]
            loads.append(pltpu.make_async_copy(src, dst, load_sem.at[7 + 2 * d + half]))
    sp = lax.axis_index("sp")
    tx = lax.axis_index("tp")
    core = sp % 2
    yy = (sp // 2) % 4
    zz = sp // 8

    def at(y, z, c):
        return (z % 4) * 8 + (y % 4) * 2 + c

    sib = at(yy, zz, 1 - core)
    y_next, y_prev = at(yy + 1, zz, core), at(yy + 3, zz, core)
    z_next, z_prev = at(yy, zz + 1, core), at(yy, zz + 3, core)

    mine = (tx, yy, zz)
    place_of = (sp, zz * 8 + core * 4 + tx, yy * 8 + core * 4 + tx)

    def plane_device(d, q):
        if d == 0:
            return (q, tx)
        c, x = (q // 4) % 2, q % 4
        if d == 1:
            return ((q // 8) * 8 + yy * 2 + c, x)
        return (zz * 8 + (q // 8) * 2 + c, x)

    def ring_device(d, j):
        if d == 0:
            return (sp, j)
        if d == 1:
            return (at(j, zz, core), tx)
        return (at(yy, j, core), tx)

    barrier = pltpu.get_barrier_semaphore()
    for d in range(3):

        def greet(i, carry, d=d):
            peer = plane_device(d, (place_of[d] + i) % 32)
            pl.semaphore_signal(barrier, inc=1, device_id=peer, device_id_type=MESH)
            return carry

        lax.fori_loop(1, 32, greet, 0)

    counter = [0]
    sent = []

    def push(kind, slot, peer):
        buf, recv = (kt_all, krecv) if kind == 0 else (v_all, vrecv)
        copy = pltpu.make_async_remote_copy(
            src_ref=buf.at[slot],
            dst_ref=buf.at[slot],
            send_sem=send_sem.at[counter[0]],
            recv_sem=recv.at[slot],
            device_id=(peer, tx),
            device_id_type=MESH,
        )
        sent.append((kind, counter[0]))
        counter[0] += 1
        copy.start()

    def arrived(kind, slot):
        buf, recv = (kt_all, krecv) if kind == 0 else (v_all, vrecv)
        pltpu.make_async_remote_copy(
            src_ref=buf.at[slot],
            dst_ref=buf.at[slot],
            send_sem=send_sem.at[0],
            recv_sem=recv.at[slot],
            device_id=(sib, tx),
            device_id_type=MESH,
        ).wait_recv()

    def origin(dy, dz, c):
        return at(yy - dy + 4, zz - dz + 4, c)

    for r in range(8):
        sl = pl.ds(r * GRID_W, GRID_W)
        for i in range(2):
            trig[i, sl, :] = rows_ref[i, pl.ds(sp * 8 + r, 1), :] + cols_ref[i]

    kr = normed_rotary(k_ref[...], kg_ref[...], trig[0], trig[1])
    kt_all[sp] = kr.T.astype(BF16)
    v_all[sp] = v_ref[...]
    pl.semaphore_wait(barrier, 93)
    for kind in (0, 1):
        for peer in (y_next, y_prev, z_next, z_prev):
            push(kind, sp, peer)
    push(0, sp, sib)
    push(1, sp, sib)
    for load in loads:
        load.start()

    lane = lax.broadcasted_iota(jnp.int32, (128, 128), 1)
    sub = lax.broadcasted_iota(jnp.int32, (128, 128), 0)
    named = [routes_ref[:, k : k + 1] for k in range(4)]
    hot = [(named[k] == lane).astype(F32) for k in range(4)]
    every = (hot[0] + hot[1] + hot[2] + hot[3]).astype(BF16)
    before = jnp.dot((lane < sub).astype(BF16), every, preferred_element_type=F32)
    table = jnp.zeros((128, 128), F32)
    for k in range(4):
        rank = jnp.sum(hot[k] * before, axis=1, keepdims=True)
        table = jnp.where(lane == k, named[k].astype(F32) * 8.0 + rank, table)
        table = jnp.where(lane == 4 + k, rweight_ref[:, k : k + 1], table)
    table = table.T[0:8, :]
    for d in range(3):
        meta[d, mine[d]] = table

    def ring_copy(buf, dst, d, i, phase):
        j = (mine[d] + i) % 4
        if dst is None:
            source, target = buf.at[mine[d]], buf.at[mine[d]]
        else:
            source, target = buf.at[j], dst.at[mine[d]]
        return pltpu.make_async_remote_copy(
            src_ref=source,
            dst_ref=target,
            send_sem=ring_send.at[phase, d, i],
            recv_sem=ring_recv.at[phase, d, mine[d]],
            device_id=ring_device(d, j),
            device_id_type=MESH,
        )

    def ring_arrived(buf, d, i, phase):
        j = (mine[d] + i) % 4
        pltpu.make_async_remote_copy(
            src_ref=buf.at[j],
            dst_ref=buf.at[j],
            send_sem=ring_send.at[phase, d, i],
            recv_sem=ring_recv.at[phase, d, j],
            device_id=ring_device(d, j),
            device_id_type=MESH,
        ).wait_recv()

    for d in range(3):
        for i in (1, 2, 3):
            ring_copy(meta.at[d], None, d, i, 0).start()

    factor = math.log2(math.e) / math.sqrt(HD)
    for h in range(4):
        qr = normed_rotary(q_ref[:, h * HD : (h + 1) * HD], qg_ref[...], trig[0], trig[1])
        qs = qr.astype(BF16).astype(F32) * factor
        hi = qs.astype(BF16)
        q_hl[h * TOK : (h + 1) * TOK, 0:HD] = hi
        q_hl[h * TOK : (h + 1) * TOK, HD : 2 * HD] = (qs - hi.astype(F32)).astype(BF16)
    acc[...] = jnp.zeros_like(acc)
    mstate[...] = jnp.full_like(mstate, -1e30)

    def attend(slots):
        n = len(slots)
        width = n * TOK
        kt = jnp.concatenate([kt_all[s] for s in slots], axis=1)
        k2 = jnp.concatenate([kt, kt], axis=0)
        vv = jnp.concatenate([v_all[s] for s in slots], axis=0)
        v2 = jnp.concatenate([vv, jnp.ones_like(vv)], axis=1)

        def scores(h):
            return jnp.dot(
                q_hl[h * TOK : (h + 1) * TOK, :], k2, preferred_element_type=F32
            )

        s = scores(0)
        for h in range(4):
            sl = slice(h * TOK, (h + 1) * TOK)
            old = mstate[sl, :]
            top = s[:, 0:HD]
            for j in range(1, width // HD):
                top = jnp.maximum(top, s[:, j * HD : (j + 1) * HD])
            new = jnp.maximum(old, jnp.max(top, axis=1, keepdims=True))
            mstate[sl, :] = new
            p = jnp.exp2(s - new[:, 0:1]).astype(BF16)
            if h < 3:
                s = scores(h + 1)
            shrink = jnp.exp2(old - new)
            pv = jnp.dot(p, v2, preferred_element_type=F32)
            acc[sl, :] = acc[sl, :] * jnp.concatenate([shrink, shrink], axis=1) + pv

    def pair_arrived(dy, dz, c):
        slot = origin(dy, dz, c)
        arrived(0, slot)
        arrived(1, slot)

    def to_sibling(group):
        for dy, dz in group:
            slot = origin(dy, dz, core)
            push(0, slot, sib)
            push(1, slot, sib)

    arrived(0, sib)
    arrived(1, sib)
    attend([sp, sib])

    def event(t):
        if t == 0:
            for dy, dz in A_SET:
                pair_arrived(dy, dz, core)
            turn = 1 + 2 * core
            for d in (1, 3):
                push(0, origin(d, 0, core), z_next)
                push(0, origin(d, 0, core), z_prev)
                push(1, origin(0, d, core), y_next)
                push(1, origin(0, d, core), y_prev)
            push(0, origin(turn, 0, core), at(yy + turn, zz, core))
            push(1, origin(0, turn, core), at(yy, zz + turn, core))
            push(0, origin(0, 1, core), z_next)
            push(1, origin(1, 0, core), y_next)
            to_sibling(A_SET)
        if t == 1:
            for dy, dz in A_SET:
                pair_arrived(dy, dz, 1 - core)
        if t == 2:
            for dy, dz in B_SET + C_SET:
                pair_arrived(dy, dz, core)
            push(0, origin(2, 0, core), z_next)
            push(0, origin(2, 0, core), z_prev)
            push(1, origin(0, 2, core), y_next)
            push(1, origin(0, 2, core), y_prev)
            push(0, origin(1, 1, core), z_next)
            push(0, origin(3, 3, core), z_prev)
            push(1, origin(1, 1, core), y_next)
            push(1, origin(3, 3, core), y_prev)
            to_sibling(B_SET + C_SET)
        if t == 3:
            for dy, dz in B_SET:
                pair_arrived(dy, dz, 1 - core)
        if t == 4:
            for dy, dz in D_SET:
                pair_arrived(dy, dz, core)
            push(0, origin(2, 3, core), z_prev)
            push(1, origin(3, 2, core), y_prev)
            to_sibling(D_SET)
            for dy, dz in C_SET:
                pair_arrived(dy, dz, 1 - core)
        if t == 5:
            pair_arrived(2, 2, core)
            to_sibling(E_SET)
        if t == 6:
            for dy, dz in D_SET:
                pair_arrived(dy, dz, 1 - core)

    groups = (
        [(dy, dz, 0) for dy, dz in A_SET],
        [(dy, dz, 1) for dy, dz in A_SET],
        [(dy, dz, 0) for dy, dz in B_SET],
        [(dy, dz, 1) for dy, dz in B_SET],
        [(2, 0, 0), (0, 2, 0), (2, 0, 1), (0, 2, 1)],
        [(dy, dz, 0) for dy, dz in D_SET],
        [(dy, dz, 1) for dy, dz in D_SET],
    )

    def chosen(values, t):
        code = sum(v * 4**i for i, v in enumerate(values))
        out = (code >> (2 * t)) % 4
        return out

    def one_step(t, carry):
        for i in range(7):

            @pl.when(t == i)
            def _(i=i):
                event(i)

        slots = []
        for j in range(4):
            dy = chosen([g[j][0] for g in groups], t)
            dz = chosen([g[j][1] for g in groups], t)
            flip = chosen([g[j][2] for g in groups], t)
            slots.append(origin(dy, dz, (core + flip) % 2))
        attend(slots)
        return carry

    lax.fori_loop(0, 7, one_step, 0)
    pair_arrived(2, 2, 1 - core)
    attend([origin(2, 2, core), origin(2, 2, 1 - core)])

    for h in range(4):
        sl = slice(h * TOK, (h + 1) * TOK)
        o = (acc[sl, 0:HD] / acc[sl, HD : 2 * HD]).astype(BF16)
        for j in range(4):
            o_tok[j, :, h * HD : (h + 1) * HD] = o[j * 128 : (j + 1) * 128, :]
    exchanges = []
    for step in (1, 2, 3):
        peer = (tx + step) % 4
        copy = pltpu.make_async_remote_copy(
            src_ref=o_tok.at[peer],
            dst_ref=hx_ref.at[tx],
            send_sem=send_sem.at[counter[0]],
            recv_sem=xrecv.at[tx],
            device_id=(sp, peer),
            device_id_type=MESH,
        )
        counter[0] += 1
        copy.start()
        exchanges.append(copy)
    hx_ref[tx] = o_tok[tx]
    for d in range(3):
        for i in (1, 2, 3):
            ring_arrived(meta.at[d], d, i, 0)

    def expert_of(d, q):
        if d == 0:
            return q * 4 + tx
        c, x = (q >> 2) & 1, q & 3
        if d == 1:
            return ((q >> 3) * 8 + yy * 2 + c) * 4 + x
        return (zz * 8 + (q >> 3) * 2 + c) * 4 + x

    def wanted(d, r):
        return (expert_of(d, r >> 4) * 8 + (r & 7) + ((r >> 3) & 1) * 4096).astype(F32)

    for d in range(3):
        want = wanted(d, lax.broadcasted_iota(jnp.int32, (512, 256), 0))
        for pair in range(2):
            first, second = meta[d, 2 * pair], meta[d, 2 * pair + 1]
            hit = None
            for k in range(4):
                have = jnp.concatenate(
                    [first[k : k + 1, :], second[k : k + 1, :] + 4096.0], axis=1
                )
                one = want == have
                hit = one if hit is None else hit | one
            place[d, pair] = jnp.where(hit, 1.0, 0.0).astype(BF16)
    loads[0].wait()
    for load in loads[7:]:
        load.wait()
    for step in (1, 2, 3):
        source = (tx + step) % 4
        pltpu.make_async_remote_copy(
            src_ref=o_tok.at[source],
            dst_ref=hx_ref.at[source],
            send_sem=send_sem.at[0],
            recv_sem=xrecv.at[source],
            device_id=(sp, source),
            device_id_type=MESH,
        ).wait_recv()
    for copy in exchanges:
        copy.wait_send()
    for kind, index in sent:
        buf, recv = (kt_all, krecv) if kind == 0 else (v_all, vrecv)
        pltpu.make_async_remote_copy(
            src_ref=buf.at[sp],
            dst_ref=buf.at[sp],
            send_sem=send_sem.at[index],
            recv_sem=recv.at[sp],
            device_id=(sib, tx),
            device_id_type=MESH,
        ).wait_send()

    heads = jnp.concatenate([hx_ref[j] for j in range(4)], axis=1)
    square = jnp.zeros((128, 128), F32)
    for d in range(3):
        lo, hi = COLS[d]
        weight = jnp.concatenate(
            [back[d][...].reshape(1024, hi - lo), sending[d][...].reshape(1024, hi - lo)], axis=0
        )
        part = jnp.dot(heads, weight, preferred_element_type=F32)
        h1 = (residual[:, lo:hi].astype(F32) + part).astype(BF16)
        hidden[:, lo:hi] = h1
        hf = h1.astype(F32)
        hf = hf * hf
        for j in range((hi - lo) // 128):
            square = square + hf[:, j * 128 : (j + 1) * 128]
    scale = lax.rsqrt(jnp.sum(square, axis=1, keepdims=True) * (1.0 / 2048.0) + EPS)
    for d in range(3):
        lo, hi = COLS[d]
        near[d][mine[d]] = (hidden[:, lo:hi].astype(F32) * scale * ng_ref[:, lo:hi]).astype(BF16)
        for i in (1, 2, 3):
            ring_copy(near[d], None, d, i, 1).start()

    def plane_copy(d, i, phase):
        q = (place_of[d] + i) % 32
        return pltpu.make_async_remote_copy(
            src_ref=sending[d].at[q],
            dst_ref=(got, back)[phase][d].at[place_of[d]],
            send_sem=plane_send.at[phase, d, i],
            recv_sem=plane_recv.at[phase, d, place_of[d]],
            device_id=plane_device(d, q),
            device_id_type=MESH,
        )

    def plane_arrived(d, q, phase):
        buf = (got, back)[phase][d]

        @pl.when(q != place_of[d])
        def _():
            pltpu.make_async_remote_copy(
                src_ref=buf.at[q],
                dst_ref=buf.at[q],
                send_sem=plane_send.at[phase, d, 0],
                recv_sem=plane_recv.at[phase, d, q],
                device_id=plane_device(d, (place_of[d] + 1) % 32),
                device_id_type=MESH,
            ).wait_recv()

    def each(lo, hi, act):
        def go(i, carry):
            act(i)
            return carry

        lax.fori_loop(lo, hi, go, 0)

    for d in range(3):
        width = COLS[d][1] - COLS[d][0]
        for i in (1, 2, 3):
            ring_arrived(near[d], d, i, 1)
        for pair in range(2):
            rows = near[d][2 * pair : 2 * pair + 2].reshape(256, width)
            moved = jnp.dot(place[d, pair], rows, preferred_element_type=F32).astype(BF16)
            sending[d][:, pair * 16 : (pair + 1) * 16, :] = moved.reshape(32, 16, width)
        each(1, 32, lambda i, d=d: plane_copy(d, i, 0).start())
        got[d][place_of[d]] = sending[d][place_of[d]]

    for load in loads[1:7]:
        load.wait()
    gpart = jnp.zeros((128, 256), F32)
    upart = jnp.zeros((128, 256), F32)
    for d in range(3):
        lo, hi = COLS[d]
        rows = near[d][mine[d]]
        gpart = gpart + jnp.dot(rows, sgate[lo:hi, :], preferred_element_type=F32)
        upart = upart + jnp.dot(rows, sup[lo:hi, :], preferred_element_type=F32)
    shid = (jax.nn.silu(gpart) * upart).astype(BF16)
    for cb in range(4):
        sl = slice(cb * 512, (cb + 1) * 512)
        shared[:, sl] = jnp.dot(shid, sdown[:, sl], preferred_element_type=F32)

    def block_of(d, q, j):
        if d == 0:
            return q * 4 + j
        c, x = (q // 4) % 2, q % 4
        if d == 1:
            return (q // 8) * 32 + j * 8 + c * 4 + x
        return j * 32 + (q // 8) * 8 + c * 4 + x

    for g in range(4):
        for d in range(3):
            lo, hi = COLS[d]
            each(g * 8, g * 8 + 8, lambda q, d=d: plane_arrived(d, q, 0))
            rows = got[d][g * 8 : g * 8 + 8].reshape(256, hi - lo)
            for n, weight in enumerate((gate, up)):
                part = jnp.dot(rows, weight[lo:hi, :], preferred_element_type=F32)
                for qi in range(8):
                    for j in range(4):
                        at_row = (qi * 4 + j) * 8
                        b = block_of(d, g * 8 + qi, j)
                        piece = part[at_row : at_row + 8, :]
                        if d == 0:
                            gsum[0, n, b] = piece
                        elif d == 1:
                            gsum[0, n, b] = gsum[0, n, b] + piece
                        else:
                            gsum[1, n, b] = piece
    for z in range(4):
        sl = slice(z * 32, (z + 1) * 32)
        gg = (gsum[0, 0, sl] + gsum[1, 0, sl]).reshape(256, 256)
        uu = (gsum[0, 1, sl] + gsum[1, 1, sl]).reshape(256, 256)
        hsum[sl] = (jax.nn.silu(gg) * uu).reshape(32, 8, 256)
    for d in range(3):
        each(1, 32, lambda i, d=d: plane_copy(d, i, 0).wait_send())
    for d in range(3):
        lo, hi = COLS[d]
        for g in range(4):
            rows = jnp.concatenate(
                [hsum[block_of(d, g * 8 + qi, j)] for qi in range(8) for j in range(4)], axis=0
            ).astype(BF16)
            result = jnp.dot(rows, down[:, lo:hi], preferred_element_type=F32).astype(BF16)
            sending[d][g * 8 : g * 8 + 8] = result.reshape(8, 32, hi - lo)
        each(1, 32, lambda i, d=d: plane_copy(d, i, 1).start())
        back[d][place_of[d]] = sending[d][place_of[d]]

    for d in range(3):
        for i in (1, 2, 3):
            ring_copy(near[d], None, d, i, 1).wait_send()
            ring_copy(meta.at[d], None, d, i, 0).wait_send()
    for d in range(3):
        want = wanted(d, lax.broadcasted_iota(jnp.int32, (256, 512), 1))
        for pair in range(2):
            both = jnp.concatenate([meta[d, 2 * pair], meta[d, 2 * pair + 1]], axis=1)
            tall = jnp.concatenate([both, jnp.zeros((120, 256), F32)], axis=0).T
            shift = (lax.broadcasted_iota(jnp.int32, (256, 1), 0) >> 7).astype(F32) * 4096.0
            total = jnp.zeros((256, 512), F32)
            for k in range(4):
                total = jnp.where(
                    want == tall[:, k : k + 1] + shift, tall[:, 4 + k : 5 + k], total
                )
            total = total.astype(BF16)
            mixw[d, pair] = total

    for d in range(3):
        lo, hi = COLS[d]
        width = hi - lo
        each(0, 32, lambda q, d=d: plane_arrived(d, q, 1))
        for pair in range(2):
            rows = back[d][:, pair * 16 : (pair + 1) * 16, :].reshape(512, width)
            part = jnp.dot(mixw[d, pair], rows, preferred_element_type=F32).astype(BF16)
            near[d][2 * pair : 2 * pair + 2] = part.reshape(2, 128, width)
        for i in (1, 2, 3):
            ring_copy(near[d], fin[d], d, i, 2).start()
        fin[d][mine[d]] = near[d][mine[d]]
    for d in range(3):
        lo, hi = COLS[d]
        for i in (1, 2, 3):
            ring_arrived(fin[d], d, i, 2)
        total = hidden[:, lo:hi].astype(F32) + shared[:, lo:hi]
        for j in range(4):
            total = total + fin[d][j].astype(F32)
        out_ref[:, lo:hi] = total.astype(BF16)
    for d in range(3):
        for i in (1, 2, 3):
            ring_copy(near[d], fin[d], d, i, 2).wait_send()
        each(1, 32, lambda i, d=d: plane_copy(d, i, 1).wait_send())


def layer(*operands):
    rows, cols = rotary_tables()
    vmem = pl.BlockSpec(memory_space=pltpu.VMEM)
    hbm = pl.BlockSpec(memory_space=pl.ANY)
    widths = [hi - lo for lo, hi in COLS]
    weight = pltpu.VMEM((2048, 256), BF16)
    return pl.pallas_call(
        layer_kernel,
        out_shape=jax.ShapeDtypeStruct((128, 2048), BF16),
        in_specs=[vmem] * 10 + [hbm] * 8,
        out_specs=vmem,
        scratch_shapes=[
            pltpu.VMEM((4, 128, 512), BF16),
            pltpu.VMEM((32, HD, TOK), BF16),
            pltpu.VMEM((32, TOK, HD), BF16),
            pltpu.VMEM((4 * TOK, 2 * HD), BF16),
            pltpu.VMEM((2, TOK, HD), F32),
            pltpu.VMEM((4 * TOK, 2 * HD), F32),
            pltpu.VMEM((4 * TOK, HD), F32),
            pltpu.VMEM((4, 128, 4 * HD), BF16),
            pltpu.VMEM((128, 2048), BF16),
            weight,
            weight,
            pltpu.VMEM((256, 2048), BF16),
            weight,
            weight,
            pltpu.VMEM((256, 2048), BF16),
            pltpu.VMEM((128, 2048), BF16),
            pltpu.VMEM((128, 2048), F32),
            pltpu.VMEM((3, 4, 8, 128), F32),
            pltpu.VMEM((3, 2, 512, 256), BF16),
            pltpu.VMEM((3, 2, 256, 512), BF16),
        ]
        + [pltpu.VMEM((4, 128, w), BF16) for w in widths]
        + [pltpu.VMEM((32, 32, w), BF16) for w in widths * 3]
        + [pltpu.VMEM((4, 128, w), BF16) for w in widths]
        + [
            pltpu.VMEM((2, 2, 128, 8, 256), F32),
            pltpu.VMEM((128, 8, 256), F32),
            pltpu.SemaphoreType.DMA((72,)),
            pltpu.SemaphoreType.DMA((32,)),
            pltpu.SemaphoreType.DMA((32,)),
            pltpu.SemaphoreType.DMA((4,)),
            pltpu.SemaphoreType.DMA((13,)),
            pltpu.SemaphoreType.DMA((3, 3, 4)),
            pltpu.SemaphoreType.DMA((3, 3, 4)),
            pltpu.SemaphoreType.DMA((2, 3, 32)),
            pltpu.SemaphoreType.DMA((2, 3, 32)),
        ],
        compiler_params=pltpu.CompilerParams(
            collective_id=0, has_side_effects=True, vmem_limit_bytes=67043328
        ),
        name="layer",
    )(*operands[:5], jnp.asarray(rows), jnp.asarray(cols), *operands[5:])


def body(
    queries,
    keys,
    values,
    residual,
    out_proj,
    query_gain,
    key_gain,
    norm_gain,
    routes,
    route_weight,
    expert_gate,
    expert_up,
    expert_down,
    shared_gate,
    shared_up,
    shared_down,
):
    return layer(
        queries,
        keys,
        values,
        query_gain.reshape(1, HD),
        key_gain.reshape(1, HD),
        norm_gain.reshape(1, 2048),
        routes,
        route_weight,
        residual,
        out_proj.reshape(64, 32, 2048),
        expert_gate,
        expert_up,
        expert_down,
        shared_gate,
        shared_up,
        shared_down,
    )


def solution(mesh):
    placed = (
        P("sp", "tp"),
        P("sp", "tp"),
        P("sp", "tp"),
        P(("sp", "tp"), None),
        P(),
        P(),
        P(),
        P(),
        P(("sp", "tp"), None),
        P(("sp", "tp"), None),
        P(("sp", "tp"), None, None),
        P(("sp", "tp"), None, None),
        P(("sp", "tp"), None, None),
        P(),
        P(),
        P(),
    )
    return jax.shard_map(
        body, mesh=mesh, in_specs=placed, out_specs=P(("sp", "tp"), None), check_vma=False
    )
```

```python
import math

import jax
import jax.numpy as jnp
import numpy as np
from jax import lax
from jax.experimental import pallas as pl
from jax.experimental.pallas import tpu as pltpu
from jax.sharding import PartitionSpec as P

HEADS = 16
KV_HEADS = 4
GRID_W = 64
HD = 128
TOK = 512
EPS = 1e-06
THETA = 10000.0
MESH = pl.DeviceIdType.MESH
F32 = jnp.float32
BF16 = jnp.bfloat16


def rotary_tables():
    quarter = HD // 4
    inverse = (THETA ** (-4.0 * np.arange(quarter, dtype=np.float64) / HD)).astype(np.float32)

    def table(count):
        angle = np.arange(count, dtype=np.float32)[:, None] * inverse[None, :]
        angle = angle.astype(np.float32).astype(np.float64)
        cosine = np.cos(angle).astype(np.float32)
        sine = np.sin(angle).astype(np.float32)
        return np.concatenate([cosine, cosine], 1), np.concatenate([-sine, sine], 1)

    row_cos, row_sin = table(256)
    col_cos, col_sin = table(GRID_W)
    zr, zc = np.zeros_like(row_cos), np.zeros_like(col_cos)
    rows = np.stack([np.concatenate([row_cos, zr], 1), np.concatenate([row_sin, zr], 1)])
    cols = np.stack([np.concatenate([zc, col_cos], 1), np.concatenate([zc, col_sin], 1)])
    return rows, cols


def normed_rotary(source, gain, cos_t, sin_t):
    x = source.astype(F32)
    x = x * lax.rsqrt(jnp.mean(x * x, axis=-1, keepdims=True) + EPS) * gain
    lane = lax.broadcasted_iota(jnp.int32, x.shape, 1)
    partner = jnp.where((lane // 32) % 2 == 0, pltpu.roll(x, 96, 1), pltpu.roll(x, 32, 1))
    return x * cos_t + partner * sin_t


A_SET = ((1, 0), (3, 0), (0, 1), (0, 3))
B_SET = ((1, 1), (1, 3), (3, 1), (3, 3))
C_SET = ((2, 0), (0, 2))
D_SET = ((2, 1), (2, 3), (1, 2), (3, 2))
E_SET = ((2, 2),)


def far(a):
    return 2 if a == 2 else a % 2


PLANE = [(a, b, c) for a in range(4) for b in range(4) for c in range(2) if a or b or c]
FARTHEST = sorted(PLANE, key=lambda m: -far(m[0]) - far(m[1]))
GROUPED = sorted(PLANE, key=lambda m: (-far(m[0]), -far(m[1]), m[2], m[1], m[0]))
COLS = ((0, 640), (640, 1280), (1280, 2048))


def layer_kernel(
    q_ref,
    k_ref,
    v_ref,
    qg_ref,
    kg_ref,
    rows_ref,
    cols_ref,
    ng_ref,
    routes_ref,
    rweight_ref,
    residual_hbm,
    out_proj_hbm,
    gate_hbm,
    up_hbm,
    down_hbm,
    sgate_hbm,
    sup_hbm,
    sdown_hbm,
    out_ref,
    hx_ref,
    kt_all,
    v_all,
    q_hl,
    trig,
    acc,
    mstate,
    o_tok,
    residual,
    gate,
    up,
    down,
    sgate,
    sup,
    sdown,
    hidden,
    shared,
    meta,
    table_s,
    place,
    mixw,
    nbx,
    nby,
    nbz,
    sendx,
    sendy,
    sendz,
    gotx,
    goty,
    gotz,
    backx,
    backy,
    backz,
    finx,
    finy,
    finz,
    gsum,
    hsum,
    send_sem,
    krecv,
    vrecv,
    head_send,
    head_recv,
    load_sem,
    ring_send,
    ring_recv,
    plane_send,
    plane_recv,
):
    near = (nbx, nby, nbz)
    sending = (sendx, sendy, sendz)
    got = (gotx, goty, gotz)
    back = (backx, backy, backz)
    fin = (finx, finy, finz)
    loads = [
        pltpu.make_async_copy(src, dst, load_sem.at[i])
        for i, (src, dst) in enumerate(
            (
                (residual_hbm, residual),
                (gate_hbm.at[0], gate),
                (up_hbm.at[0], up),
                (down_hbm.at[0], down),
                (sgate_hbm, sgate),
                (sup_hbm, sup),
                (sdown_hbm, sdown),
            )
        )
    ]
    for d, (lo, hi) in enumerate(COLS):
        for half, dst in enumerate((back[d], sending[d])):
            src = out_proj_hbm.at[pl.ds(half * 32, 32), :, lo:hi]
            loads.append(pltpu.make_async_copy(src, dst, load_sem.at[7 + 2 * d + half]))
    sp = lax.axis_index("sp")
    tx = lax.axis_index("tp")
    core = sp % 2
    yy = (sp // 2) % 4
    zz = sp // 8

    def at(y, z, c):
        return (z % 4) * 8 + (y % 4) * 2 + c

    sib = at(yy, zz, 1 - core)
    y_next, y_prev = at(yy + 1, zz, core), at(yy + 3, zz, core)
    z_next, z_prev = at(yy, zz + 1, core), at(yy, zz + 3, core)

    mine = (tx, yy, zz)
    place_of = (sp, zz * 8 + core * 4 + tx, yy * 8 + core * 4 + tx)

    def plane_device(d, q):
        if d == 0:
            return (q, tx)
        c, x = (q // 4) % 2, q % 4
        if d == 1:
            return ((q // 8) * 8 + yy * 2 + c, x)
        return (zz * 8 + (q // 8) * 2 + c, x)

    def ring_device(d, j):
        if d == 0:
            return (sp, j)
        if d == 1:
            return (at(j, zz, core), tx)
        return (at(yy, j, core), tx)

    barrier = pltpu.get_barrier_semaphore()
    peers = [(sib, tx)] + [ring_device(d, (mine[d] + i) % 4) for d in range(3) for i in (1, 2, 3)]
    for peer in peers:
        pl.semaphore_signal(barrier, inc=1, device_id=peer, device_id_type=MESH)

    counter = [0]
    sent = []

    def push(kind, slot, peer):
        buf, recv = (kt_all, krecv) if kind == 0 else (v_all, vrecv)
        copy = pltpu.make_async_remote_copy(
            src_ref=buf.at[slot],
            dst_ref=buf.at[slot],
            send_sem=send_sem.at[counter[0]],
            recv_sem=recv.at[slot],
            device_id=(peer, tx),
            device_id_type=MESH,
        )
        sent.append((kind, counter[0]))
        counter[0] += 1
        copy.start()

    def arrived(kind, slot):
        buf, recv = (kt_all, krecv) if kind == 0 else (v_all, vrecv)
        pltpu.make_async_remote_copy(
            src_ref=buf.at[slot],
            dst_ref=buf.at[slot],
            send_sem=send_sem.at[0],
            recv_sem=recv.at[slot],
            device_id=(sib, tx),
            device_id_type=MESH,
        ).wait_recv()

    def origin(dy, dz, c):
        return at(yy - dy + 4, zz - dz + 4, c)

    for r in range(8):
        sl = pl.ds(r * GRID_W, GRID_W)
        for i in range(2):
            trig[i, sl, :] = rows_ref[i, pl.ds(sp * 8 + r, 1), :] + cols_ref[i]

    kr = normed_rotary(k_ref[...], kg_ref[...], trig[0], trig[1])
    kt_all[sp] = kr.T.astype(BF16)
    v_all[sp] = v_ref[...]
    factor = math.log2(math.e) / math.sqrt(HD)
    for h in range(4):
        qr = normed_rotary(q_ref[:, h * HD : (h + 1) * HD], qg_ref[...], trig[0], trig[1])
        qs = qr.astype(BF16).astype(F32) * factor
        hi = qs.astype(BF16)
        q_hl[h * TOK : (h + 1) * TOK, 0:HD] = hi
        q_hl[h * TOK : (h + 1) * TOK, HD : 2 * HD] = (qs - hi.astype(F32)).astype(BF16)
    acc[...] = jnp.zeros_like(acc)
    mstate[...] = jnp.full_like(mstate, -1e30)

    def ring_copy(buf, dst, d, i, phase):
        j = (mine[d] + i) % 4
        if dst is None:
            source, target = buf.at[mine[d]], buf.at[mine[d]]
        else:
            source, target = buf.at[j], dst.at[mine[d]]
        return pltpu.make_async_remote_copy(
            src_ref=source,
            dst_ref=target,
            send_sem=ring_send.at[phase, d, i],
            recv_sem=ring_recv.at[phase, d, mine[d]],
            device_id=ring_device(d, j),
            device_id_type=MESH,
        )

    def ring_arrived(buf, d, i, phase):
        j = (mine[d] + i) % 4
        pltpu.make_async_remote_copy(
            src_ref=buf.at[j],
            dst_ref=buf.at[j],
            send_sem=ring_send.at[phase, d, i],
            recv_sem=ring_recv.at[phase, d, j],
            device_id=ring_device(d, j),
            device_id_type=MESH,
        ).wait_recv()

    pl.semaphore_wait(barrier, 10)
    for kind in (0, 1):
        for peer in (y_next, y_prev, z_next, z_prev):
            push(kind, sp, peer)
    push(0, sp, sib)
    push(1, sp, sib)
    for load in loads:
        load.start()

    lane = lax.broadcasted_iota(jnp.int32, (128, 128), 1)
    sub = lax.broadcasted_iota(jnp.int32, (128, 128), 0)
    table_s[...] = jnp.zeros((128, 128), F32)
    table_s[0:4, :] = routes_ref[...].astype(F32)
    table_s[4:8, :] = rweight_ref[...]
    tall = table_s[...].T
    hot = [(tall[:, k : k + 1] == lane.astype(F32)).astype(F32) for k in range(4)]
    every = (hot[0] + hot[1] + hot[2] + hot[3]).astype(BF16)
    before = jnp.dot((lane < sub).astype(BF16), every, preferred_element_type=F32)
    table = jnp.where(lane < 8, tall, 0.0)
    for k in range(4):
        rank = jnp.sum(hot[k] * before, axis=1, keepdims=True)
        table = jnp.where(lane == k, tall[:, k : k + 1] * 8.0 + rank, table)
    table = table.T[0:8, :]
    for d in range(3):
        meta[d, mine[d]] = table
    for d in range(3):
        for i in (1, 2, 3):
            ring_copy(meta.at[d], None, d, i, 0).start()

    def head_rows(h):
        return pl.ds(pl.multiple_of(h * TOK, TOK), TOK)

    def attend(slots, heads=(0, 1, 2, 3)):
        n = len(slots)
        width = n * TOK
        kt = jnp.concatenate([kt_all[s] for s in slots], axis=1)
        k2 = jnp.concatenate([kt, kt], axis=0)
        vv = jnp.concatenate([v_all[s] for s in slots], axis=0)
        v2 = jnp.concatenate([vv, jnp.ones_like(vv)], axis=1)

        def scores(h):
            return jnp.dot(q_hl[head_rows(h), :], k2, preferred_element_type=F32)

        s = scores(heads[0])
        for i, h in enumerate(heads):
            sl = head_rows(h)
            old = mstate[sl, :]
            top = s[:, 0:HD]
            for j in range(1, width // HD):
                top = jnp.maximum(top, s[:, j * HD : (j + 1) * HD])
            new = jnp.maximum(old, jnp.max(top, axis=1, keepdims=True))
            mstate[sl, :] = new
            p = jnp.exp2(s - new[:, 0:1]).astype(BF16)
            if i + 1 < len(heads):
                s = scores(heads[i + 1])
            shrink = jnp.exp2(old - new)
            pv = jnp.dot(p, v2, preferred_element_type=F32)
            acc[sl, :] = acc[sl, :] * jnp.concatenate([shrink, shrink], axis=1) + pv

    def pair_arrived(dy, dz, c):
        slot = origin(dy, dz, c)
        arrived(0, slot)
        arrived(1, slot)

    def to_sibling(group):
        for dy, dz in group:
            slot = origin(dy, dz, core)
            push(0, slot, sib)
            push(1, slot, sib)

    arrived(0, sib)
    arrived(1, sib)
    attend([sp, sib])

    for d in range(3):
        for i in (1, 2, 3):
            ring_arrived(meta.at[d], d, i, 0)

    def expert_of(d, q):
        if d == 0:
            return q * 4 + tx
        c, x = (q >> 2) & 1, q & 3
        if d == 1:
            return ((q >> 3) * 8 + yy * 2 + c) * 4 + x
        return (zz * 8 + (q >> 3) * 2 + c) * 4 + x

    def wanted(d, r):
        return (expert_of(d, r >> 4) * 8 + (r & 7) + ((r >> 3) & 1) * 4096).astype(F32)

    for d in range(3):
        want = wanted(d, lax.broadcasted_iota(jnp.int32, (512, 256), 0))
        for pair in range(2):
            first, second = meta[d, 2 * pair], meta[d, 2 * pair + 1]
            hit = None
            for k in range(4):
                have = jnp.concatenate(
                    [first[k : k + 1, :], second[k : k + 1, :] + 4096.0], axis=1
                )
                one = want == have
                hit = one if hit is None else hit | one
            place[d, pair] = jnp.where(hit, 1.0, 0.0).astype(BF16)
    for d in range(3):
        want = wanted(d, lax.broadcasted_iota(jnp.int32, (256, 512), 1))
        for pair in range(2):
            both = jnp.concatenate([meta[d, 2 * pair], meta[d, 2 * pair + 1]], axis=1)
            tall = jnp.concatenate([both, jnp.zeros((120, 256), F32)], axis=0).T
            shift = (lax.broadcasted_iota(jnp.int32, (256, 1), 0) >> 7).astype(F32) * 4096.0
            total = jnp.zeros((256, 512), F32)
            for k in range(4):
                total = jnp.where(
                    want == tall[:, k : k + 1] + shift, tall[:, 4 + k : 5 + k], total
                )
            total = total.astype(BF16)
            mixw[d, pair] = total

    def event(t):
        if t == 0:
            for dy, dz in A_SET:
                pair_arrived(dy, dz, core)
            turn = 1 + 2 * core
            for d in (1, 3):
                push(0, origin(d, 0, core), z_next)
                push(0, origin(d, 0, core), z_prev)
                push(1, origin(0, d, core), y_next)
                push(1, origin(0, d, core), y_prev)
            push(0, origin(turn, 0, core), at(yy + turn, zz, core))
            push(1, origin(0, turn, core), at(yy, zz + turn, core))
            push(0, origin(0, 1, core), z_next)
            push(1, origin(1, 0, core), y_next)
            to_sibling(A_SET)
        if t == 1:
            for dy, dz in A_SET:
                pair_arrived(dy, dz, 1 - core)
        if t == 2:
            for dy, dz in B_SET + C_SET:
                pair_arrived(dy, dz, core)
            push(0, origin(2, 0, core), z_next)
            push(0, origin(2, 0, core), z_prev)
            push(1, origin(0, 2, core), y_next)
            push(1, origin(0, 2, core), y_prev)
            push(0, origin(1, 1, core), z_next)
            push(0, origin(3, 3, core), z_prev)
            push(1, origin(1, 1, core), y_next)
            push(1, origin(3, 3, core), y_prev)
            to_sibling(B_SET + C_SET)
        if t == 3:
            for dy, dz in B_SET:
                pair_arrived(dy, dz, 1 - core)
        if t == 4:
            for dy, dz in D_SET:
                pair_arrived(dy, dz, core)
            push(0, origin(2, 3, core), z_prev)
            push(1, origin(3, 2, core), y_prev)
            to_sibling(D_SET)
            for dy, dz in C_SET:
                pair_arrived(dy, dz, 1 - core)
        if t == 5:
            pair_arrived(2, 2, core)
            to_sibling(E_SET)
        if t == 6:
            for dy, dz in D_SET:
                pair_arrived(dy, dz, 1 - core)

    groups = (
        [(dy, dz, 0) for dy, dz in A_SET],
        [(dy, dz, 1) for dy, dz in A_SET],
        [(dy, dz, 0) for dy, dz in B_SET],
        [(dy, dz, 1) for dy, dz in B_SET],
        [(2, 0, 0), (0, 2, 0), (2, 0, 1), (0, 2, 1)],
        [(dy, dz, 0) for dy, dz in D_SET],
        [(dy, dz, 1) for dy, dz in D_SET],
    )

    def chosen(values, t):
        code = sum(v * 4**i for i, v in enumerate(values))
        out = (code >> (2 * t)) % 4
        return out

    def one_step(t, carry):
        for i in range(7):

            @pl.when(t == i)
            def _(i=i):
                event(i)

        slots = []
        for j in range(4):
            dy = chosen([g[j][0] for g in groups], t)
            dz = chosen([g[j][1] for g in groups], t)
            flip = chosen([g[j][2] for g in groups], t)
            slots.append(origin(dy, dz, (core + flip) % 2))
        attend(slots)
        return carry

    lax.fori_loop(0, 6, one_step, 0)
    event(6)
    pair_arrived(2, 2, 1 - core)
    late = [origin(dy, dz, 1 - core) for dy, dz in D_SET]
    last = [origin(2, 2, core), origin(2, 2, 1 - core)]

    def head_copy(step, h, source):
        peer = (tx + step) % 4
        return pltpu.make_async_remote_copy(
            src_ref=o_tok.at[peer, h],
            dst_ref=hx_ref.at[source, h],
            send_sem=head_send.at[step, h],
            recv_sem=head_recv.at[source, h],
            device_id=(sp, peer),
            device_id_type=MESH,
        )

    def finish(pair, carry):
        heads = (2 * pair, 2 * pair + 1)
        attend(late, heads)
        attend(last, heads)
        for h in heads:
            a = acc[head_rows(h), :]
            o = (a[:, 0:HD] / a[:, HD : 2 * HD]).astype(BF16)
            for j in range(4):
                o_tok[j, h] = o[j * 128 : (j + 1) * 128, :]
            for step in (1, 2, 3):
                head_copy(step, h, tx).start()
            hx_ref[tx, h] = o_tok[tx, h]
        return carry

    lax.fori_loop(0, 2, finish, 0)
    loads[0].wait()
    for load in loads[7:]:
        load.wait()
    for h in range(4):
        for step in (1, 2, 3):
            head_copy(step, h, (tx + step) % 4).wait_recv()
    for h in range(4):
        for step in (1, 2, 3):
            head_copy(step, h, tx).wait_send()
    for kind, index in sent:
        buf, recv = (kt_all, krecv) if kind == 0 else (v_all, vrecv)
        pltpu.make_async_remote_copy(
            src_ref=buf.at[sp],
            dst_ref=buf.at[sp],
            send_sem=send_sem.at[index],
            recv_sem=recv.at[sp],
            device_id=(sib, tx),
            device_id_type=MESH,
        ).wait_send()

    heads = jnp.concatenate([hx_ref[j, h] for j in range(4) for h in range(4)], axis=1)
    square = jnp.zeros((128, 128), F32)
    for d in range(3):
        lo, hi = COLS[d]
        weight = jnp.concatenate(
            [back[d][...].reshape(1024, hi - lo), sending[d][...].reshape(1024, hi - lo)], axis=0
        )
        part = jnp.dot(heads, weight, preferred_element_type=F32)
        h1 = (residual[:, lo:hi].astype(F32) + part).astype(BF16)
        hidden[:, lo:hi] = h1
        hf = h1.astype(F32)
        hf = hf * hf
        for j in range((hi - lo) // 128):
            square = square + hf[:, j * 128 : (j + 1) * 128]
    scale = lax.rsqrt(jnp.sum(square, axis=1, keepdims=True) * (1.0 / 2048.0) + EPS)
    for d in range(3):
        lo, hi = COLS[d]
        near[d][mine[d]] = (hidden[:, lo:hi].astype(F32) * scale * ng_ref[:, lo:hi]).astype(BF16)
        for i in (1, 2, 3):
            ring_copy(near[d], None, d, i, 1).start()

    def plane_copy(d, q, i, phase):
        return pltpu.make_async_remote_copy(
            src_ref=sending[d].at[q],
            dst_ref=(got, back)[phase][d].at[place_of[d]],
            send_sem=plane_send.at[phase, d, i],
            recv_sem=plane_recv.at[phase, d, place_of[d]],
            device_id=plane_device(d, q),
            device_id_type=MESH,
        )

    def spray(order, phase):
        for i, (da, db, dc) in enumerate(order):
            c = (core + dc) % 2
            plane_copy(0, ((zz + da) % 4) * 8 + ((yy + db) % 4) * 2 + c, i, phase).start()
            plane_copy(1, ((zz + da) % 4) * 8 + c * 4 + (tx + db) % 4, i, phase).start()
            plane_copy(2, ((yy + da) % 4) * 8 + c * 4 + (tx + db) % 4, i, phase).start()

    def sprayed(phase):
        for d in range(3):

            def go(i, carry, d=d):
                plane_copy(d, (place_of[d] + 1) % 32, i, phase).wait_send()
                return carry

            lax.fori_loop(0, 31, go, 0)

    def plane_arrived(d, q, phase):
        buf = (got, back)[phase][d]

        @pl.when(q != place_of[d])
        def _():
            pltpu.make_async_remote_copy(
                src_ref=buf.at[q],
                dst_ref=buf.at[q],
                send_sem=plane_send.at[phase, d, 0],
                recv_sem=plane_recv.at[phase, d, q],
                device_id=plane_device(d, (place_of[d] + 1) % 32),
                device_id_type=MESH,
            ).wait_recv()

    def each(lo, hi, act):
        def go(i, carry):
            act(i)
            return carry

        lax.fori_loop(lo, hi, go, 0)

    for d in range(3):
        width = COLS[d][1] - COLS[d][0]
        for i in (1, 2, 3):
            ring_arrived(near[d], d, i, 1)
        for pair in range(2):
            rows = near[d][2 * pair : 2 * pair + 2].reshape(256, width)
            moved = jnp.dot(place[d, pair], rows, preferred_element_type=F32).astype(BF16)
            sending[d][:, pair * 16 : (pair + 1) * 16, :] = moved.reshape(32, 16, width)
        got[d][place_of[d]] = sending[d][place_of[d]]
    spray(GROUPED, 0)

    for load in loads[1:7]:
        load.wait()
    gpart = jnp.zeros((128, 256), F32)
    upart = jnp.zeros((128, 256), F32)
    for d in range(3):
        lo, hi = COLS[d]
        rows = near[d][mine[d]]
        gpart = gpart + jnp.dot(rows, sgate[lo:hi, :], preferred_element_type=F32)
        upart = upart + jnp.dot(rows, sup[lo:hi, :], preferred_element_type=F32)
    shid = (jax.nn.silu(gpart) * upart).astype(BF16)
    for cb in range(4):
        sl = slice(cb * 512, (cb + 1) * 512)
        shared[:, sl] = jnp.dot(shid, sdown[:, sl], preferred_element_type=F32)

    def block_of(d, g, qi, j):
        if d == 0:
            return g * 32 + qi * 4 + j
        c, x = qi // 4, qi % 4
        if d == 1:
            return g * 32 + j * 8 + c * 4 + x
        return j * 32 + g * 8 + c * 4 + x

    for step in (2, 1, 3, 0):
        for d in range(3):
            lo, hi = COLS[d]
            g = ((zz, zz, yy)[d] + step) % 4
            each(0, 8, lambda q, d=d, g=g: plane_arrived(d, g * 8 + q, 0))
            rows = got[d][pl.ds(g * 8, 8)].reshape(256, hi - lo)
            for n, weight in enumerate((gate, up)):
                part = jnp.dot(rows, weight[lo:hi, :], preferred_element_type=F32)
                for qi in range(8):
                    for j in range(4):
                        at_row = (qi * 4 + j) * 8
                        b = block_of(d, g, qi, j)
                        piece = part[at_row : at_row + 8, :]
                        if d == 0:
                            gsum[0, n, b] = piece
                        elif d == 1:
                            gsum[0, n, b] = gsum[0, n, b] + piece
                        else:
                            gsum[1, n, b] = piece
    for z in range(4):
        sl = slice(z * 32, (z + 1) * 32)
        gg = (gsum[0, 0, sl] + gsum[1, 0, sl]).reshape(256, 256)
        uu = (gsum[0, 1, sl] + gsum[1, 1, sl]).reshape(256, 256)
        hsum[sl] = (jax.nn.silu(gg) * uu).reshape(32, 8, 256)
    sprayed(0)
    for d in range(3):
        lo, hi = COLS[d]
        for g in range(4):
            rows = jnp.concatenate(
                [hsum[block_of(d, g, qi, j)] for qi in range(8) for j in range(4)], axis=0
            ).astype(BF16)
            result = jnp.dot(rows, down[:, lo:hi], preferred_element_type=F32).astype(BF16)
            sending[d][g * 8 : g * 8 + 8] = result.reshape(8, 32, hi - lo)
        back[d][place_of[d]] = sending[d][place_of[d]]
    spray(FARTHEST, 1)

    for d in range(3):
        for i in (1, 2, 3):
            ring_copy(near[d], None, d, i, 1).wait_send()
            ring_copy(meta.at[d], None, d, i, 0).wait_send()
    for d in range(3):
        lo, hi = COLS[d]
        width = hi - lo
        each(0, 32, lambda q, d=d: plane_arrived(d, q, 1))
        for pair in range(2):
            rows = back[d][:, pair * 16 : (pair + 1) * 16, :].reshape(512, width)
            part = jnp.dot(mixw[d, pair], rows, preferred_element_type=F32).astype(BF16)
            near[d][2 * pair : 2 * pair + 2] = part.reshape(2, 128, width)
        for i in (1, 2, 3):
            ring_copy(near[d], fin[d], d, i, 2).start()
        fin[d][mine[d]] = near[d][mine[d]]
    for d in range(3):
        lo, hi = COLS[d]
        for i in (1, 2, 3):
            ring_arrived(fin[d], d, i, 2)
        total = hidden[:, lo:hi].astype(F32) + shared[:, lo:hi]
        for j in range(4):
            total = total + fin[d][j].astype(F32)
        out_ref[:, lo:hi] = total.astype(BF16)
    for d in range(3):
        for i in (1, 2, 3):
            ring_copy(near[d], fin[d], d, i, 2).wait_send()
    sprayed(1)


def layer(*operands):
    rows, cols = rotary_tables()
    vmem = pl.BlockSpec(memory_space=pltpu.VMEM)
    hbm = pl.BlockSpec(memory_space=pl.ANY)
    widths = [hi - lo for lo, hi in COLS]
    weight = pltpu.VMEM((2048, 256), BF16)
    return pl.pallas_call(
        layer_kernel,
        out_shape=jax.ShapeDtypeStruct((128, 2048), BF16),
        in_specs=[vmem] * 10 + [hbm] * 8,
        out_specs=vmem,
        scratch_shapes=[
            pltpu.VMEM((4, 4, 128, HD), BF16),
            pltpu.VMEM((32, HD, TOK), BF16),
            pltpu.VMEM((32, TOK, HD), BF16),
            pltpu.VMEM((4 * TOK, 2 * HD), BF16),
            pltpu.VMEM((2, TOK, HD), F32),
            pltpu.VMEM((4 * TOK, 2 * HD), F32),
            pltpu.VMEM((4 * TOK, HD), F32),
            pltpu.VMEM((4, 4, 128, HD), BF16),
            pltpu.VMEM((128, 2048), BF16),
            weight,
            weight,
            pltpu.VMEM((256, 2048), BF16),
            weight,
            weight,
            pltpu.VMEM((256, 2048), BF16),
            pltpu.VMEM((128, 2048), BF16),
            pltpu.VMEM((128, 2048), F32),
            pltpu.VMEM((3, 4, 8, 128), F32),
            pltpu.VMEM((128, 128), F32),
            pltpu.VMEM((3, 2, 512, 256), BF16),
            pltpu.VMEM((3, 2, 256, 512), BF16),
        ]
        + [pltpu.VMEM((4, 128, w), BF16) for w in widths]
        + [pltpu.VMEM((32, 32, w), BF16) for w in widths * 3]
        + [pltpu.VMEM((4, 128, w), BF16) for w in widths]
        + [
            pltpu.VMEM((2, 2, 128, 8, 256), F32),
            pltpu.VMEM((128, 8, 256), F32),
            pltpu.SemaphoreType.DMA((72,)),
            pltpu.SemaphoreType.DMA((32,)),
            pltpu.SemaphoreType.DMA((32,)),
            pltpu.SemaphoreType.DMA((4, 4)),
            pltpu.SemaphoreType.DMA((4, 4)),
            pltpu.SemaphoreType.DMA((13,)),
            pltpu.SemaphoreType.DMA((3, 3, 4)),
            pltpu.SemaphoreType.DMA((3, 3, 4)),
            pltpu.SemaphoreType.DMA((2, 3, 32)),
            pltpu.SemaphoreType.DMA((2, 3, 32)),
        ],
        compiler_params=pltpu.CompilerParams(
            collective_id=0, has_side_effects=True, vmem_limit_bytes=67043328
        ),
        name="layer",
    )(*operands[:5], jnp.asarray(rows), jnp.asarray(cols), *operands[5:])


def body(
    queries,
    keys,
    values,
    residual,
    out_proj,
    query_gain,
    key_gain,
    norm_gain,
    routes,
    route_weight,
    expert_gate,
    expert_up,
    expert_down,
    shared_gate,
    shared_up,
    shared_down,
):
    return layer(
        queries,
        keys,
        values,
        query_gain.reshape(1, HD),
        key_gain.reshape(1, HD),
        norm_gain.reshape(1, 2048),
        routes.T,
        route_weight.T,
        residual,
        out_proj.reshape(64, 32, 2048),
        expert_gate,
        expert_up,
        expert_down,
        shared_gate,
        shared_up,
        shared_down,
    )


def solution(mesh):
    placed = (
        P("sp", "tp"),
        P("sp", "tp"),
        P("sp", "tp"),
        P(("sp", "tp"), None),
        P(),
        P(),
        P(),
        P(),
        P(("sp", "tp"), None),
        P(("sp", "tp"), None),
        P(("sp", "tp"), None, None),
        P(("sp", "tp"), None, None),
        P(("sp", "tp"), None, None),
        P(),
        P(),
        P(),
    )
    return jax.shard_map(
        body, mesh=mesh, in_specs=placed, out_specs=P(("sp", "tp"), None), check_vma=False
    )
```

```python
import math

import jax
import jax.numpy as jnp
import numpy as np
from jax import lax
from jax.experimental import pallas as pl
from jax.experimental.pallas import tpu as pltpu
from jax.sharding import PartitionSpec as P

HEADS = 16
KV_HEADS = 4
GRID_W = 64
HD = 128
TOK = 512
EPS = 1e-06
THETA = 10000.0
MESH = pl.DeviceIdType.MESH
F32 = jnp.float32
BF16 = jnp.bfloat16


def rotary_tables():
    quarter = HD // 4
    inverse = (THETA ** (-4.0 * np.arange(quarter, dtype=np.float64) / HD)).astype(np.float32)

    def table(count):
        angle = np.arange(count, dtype=np.float32)[:, None] * inverse[None, :]
        angle = angle.astype(np.float32).astype(np.float64)
        cosine = np.cos(angle).astype(np.float32)
        sine = np.sin(angle).astype(np.float32)
        return np.concatenate([cosine, cosine], 1), np.concatenate([-sine, sine], 1)

    row_cos, row_sin = table(256)
    col_cos, col_sin = table(GRID_W)
    zr, zc = np.zeros_like(row_cos), np.zeros_like(col_cos)
    rows = np.stack([np.concatenate([row_cos, zr], 1), np.concatenate([row_sin, zr], 1)])
    cols = np.stack([np.concatenate([zc, col_cos], 1), np.concatenate([zc, col_sin], 1)])
    return rows, cols


def normed_rotary(source, gain, cos_t, sin_t):
    x = source.astype(F32)
    x = x * lax.rsqrt(jnp.mean(x * x, axis=-1, keepdims=True) + EPS) * gain
    lane = lax.broadcasted_iota(jnp.int32, x.shape, 1)
    partner = jnp.where((lane // 32) % 2 == 0, pltpu.roll(x, 96, 1), pltpu.roll(x, 32, 1))
    return x * cos_t + partner * sin_t


A_SET = ((1, 0), (3, 0), (0, 1), (0, 3))
B_SET = ((1, 1), (1, 3), (3, 1), (3, 3))
C_SET = ((2, 0), (0, 2))
D_SET = ((2, 1), (2, 3), (1, 2), (3, 2))
E_SET = ((2, 2),)


def far(a):
    return 2 if a == 2 else a % 2


PLANE = [(a, b, c) for a in range(4) for b in range(4) for c in range(2) if a or b or c]
GROUPED = sorted(PLANE, key=lambda m: (-far(m[0]), -far(m[1]), m[2], m[1], m[0]))
COLS = ((0, 640), (640, 1280), (1280, 2048))


def layer_kernel(
    q_hbm,
    k_hbm,
    v_hbm,
    qg_hbm,
    kg_hbm,
    rows_hbm,
    cols_hbm,
    ng_hbm,
    routes_hbm,
    rweight_hbm,
    residual_hbm,
    out_proj_hbm,
    gate_hbm,
    up_hbm,
    down_hbm,
    sgate_hbm,
    sup_hbm,
    sdown_hbm,
    out_ref,
    q_ref,
    k_ref,
    qg_ref,
    kg_ref,
    rows_ref,
    cols_ref,
    ng_ref,
    routes_ref,
    rweight_ref,
    hx_ref,
    kt_all,
    v_all,
    q_hl,
    trig,
    acc,
    mstate,
    o_tok,
    residual,
    gate,
    up,
    down,
    sgate,
    sup,
    sdown,
    hidden,
    shared,
    meta,
    table_s,
    place,
    mixw,
    nbx,
    nby,
    nbz,
    sendx,
    sendy,
    sendz,
    gotx,
    goty,
    gotz,
    backx,
    backy,
    backz,
    finx,
    finy,
    finz,
    gsum,
    hsum,
    send_sem,
    krecv,
    vrecv,
    head_send,
    head_recv,
    load_sem,
    early_sem,
    ring_send,
    ring_recv,
    plane_send,
    plane_recv,
):
    near = (nbx, nby, nbz)
    sending = (sendx, sendy, sendz)
    got = (gotx, goty, gotz)
    back = (backx, backy, backz)
    fin = (finx, finy, finz)
    loads = [
        pltpu.make_async_copy(src, dst, load_sem.at[i])
        for i, (src, dst) in enumerate(
            (
                (residual_hbm, residual),
                (gate_hbm.at[0], gate),
                (up_hbm.at[0], up),
                (down_hbm.at[0], down),
                (sgate_hbm, sgate),
                (sup_hbm, sup),
                (sdown_hbm, sdown),
            )
        )
    ]
    for d, (lo, hi) in enumerate(COLS):
        for half, dst in enumerate((back[d], sending[d])):
            src = out_proj_hbm.at[pl.ds(half * 32, 32), :, lo:hi]
            loads.append(pltpu.make_async_copy(src, dst, load_sem.at[7 + 2 * d + half]))
    sp = lax.axis_index("sp")
    tx = lax.axis_index("tp")
    core = sp % 2
    yy = (sp // 2) % 4
    zz = sp // 8

    def at(y, z, c):
        return (z % 4) * 8 + (y % 4) * 2 + c

    sib = at(yy, zz, 1 - core)
    y_next, y_prev = at(yy + 1, zz, core), at(yy + 3, zz, core)
    z_next, z_prev = at(yy, zz + 1, core), at(yy, zz + 3, core)

    mine = (tx, yy, zz)
    place_of = (sp, zz * 8 + core * 4 + tx, yy * 8 + core * 4 + tx)

    def plane_device(d, q):
        if d == 0:
            return (q, tx)
        c, x = (q // 4) % 2, q % 4
        if d == 1:
            return ((q // 8) * 8 + yy * 2 + c, x)
        return (zz * 8 + (q // 8) * 2 + c, x)

    def ring_device(d, j):
        if d == 0:
            return (sp, j)
        if d == 1:
            return (at(j, zz, core), tx)
        return (at(yy, j, core), tx)

    barrier = pltpu.get_barrier_semaphore()
    early = [
        pltpu.make_async_copy(src, dst, early_sem.at[i])
        for i, (src, dst) in enumerate(
            (
                (k_hbm, k_ref),
                (kg_hbm, kg_ref),
                (rows_hbm.at[:, pl.ds(sp * 8, 8), :], rows_ref),
                (cols_hbm, cols_ref),
                (v_hbm, v_all.at[sp]),
                (q_hbm, q_ref),
                (qg_hbm, qg_ref),
                (routes_hbm, routes_ref),
                (rweight_hbm, rweight_ref),
                (ng_hbm, ng_ref),
            )
        )
    ]
    for load in early:
        load.start()
    peers = [(sib, tx)] + [ring_device(d, (mine[d] + i) % 4) for d in range(3) for i in (1, 2, 3)]
    for peer in peers:
        pl.semaphore_signal(barrier, inc=1, device_id=peer, device_id_type=MESH)

    counter = [0]
    sent = []

    def push(kind, slot, peer):
        buf, recv = (kt_all, krecv) if kind == 0 else (v_all, vrecv)
        copy = pltpu.make_async_remote_copy(
            src_ref=buf.at[slot],
            dst_ref=buf.at[slot],
            send_sem=send_sem.at[counter[0]],
            recv_sem=recv.at[slot],
            device_id=(peer, tx),
            device_id_type=MESH,
        )
        sent.append((kind, counter[0]))
        counter[0] += 1
        copy.start()

    def arrived(kind, slot):
        buf, recv = (kt_all, krecv) if kind == 0 else (v_all, vrecv)
        pltpu.make_async_remote_copy(
            src_ref=buf.at[slot],
            dst_ref=buf.at[slot],
            send_sem=send_sem.at[0],
            recv_sem=recv.at[slot],
            device_id=(sib, tx),
            device_id_type=MESH,
        ).wait_recv()

    def origin(dy, dz, c):
        return at(yy - dy + 4, zz - dz + 4, c)

    for load in early:
        load.wait()
    for r in range(8):
        sl = pl.ds(r * GRID_W, GRID_W)
        for i in range(2):
            trig[i, sl, :] = rows_ref[i, r : r + 1, :] + cols_ref[i]

    kr = normed_rotary(k_ref[...], kg_ref[...], trig[0], trig[1])
    kt_all[sp] = kr.T.astype(BF16)
    factor = math.log2(math.e) / math.sqrt(HD)
    for h in range(4):
        qr = normed_rotary(q_ref[:, h * HD : (h + 1) * HD], qg_ref[...], trig[0], trig[1])
        qs = qr.astype(BF16).astype(F32) * factor
        hi = qs.astype(BF16)
        q_hl[h * TOK : (h + 1) * TOK, 0:HD] = hi
        q_hl[h * TOK : (h + 1) * TOK, HD : 2 * HD] = (qs - hi.astype(F32)).astype(BF16)
    acc[...] = jnp.zeros_like(acc)
    mstate[...] = jnp.full_like(mstate, -1e30)

    def ring_copy(buf, dst, d, i, phase):
        j = (mine[d] + i) % 4
        if dst is None:
            source, target = buf.at[mine[d]], buf.at[mine[d]]
        else:
            source, target = buf.at[j], dst.at[mine[d]]
        return pltpu.make_async_remote_copy(
            src_ref=source,
            dst_ref=target,
            send_sem=ring_send.at[phase, d, i],
            recv_sem=ring_recv.at[phase, d, mine[d]],
            device_id=ring_device(d, j),
            device_id_type=MESH,
        )

    def ring_arrived(buf, d, i, phase):
        j = (mine[d] + i) % 4
        pltpu.make_async_remote_copy(
            src_ref=buf.at[j],
            dst_ref=buf.at[j],
            send_sem=ring_send.at[phase, d, i],
            recv_sem=ring_recv.at[phase, d, j],
            device_id=ring_device(d, j),
            device_id_type=MESH,
        ).wait_recv()

    pl.semaphore_wait(barrier, 10)
    for kind in (0, 1):
        for peer in (y_next, y_prev, z_next, z_prev):
            push(kind, sp, peer)
    push(0, sp, sib)
    push(1, sp, sib)
    for load in loads:
        load.start()

    lane = lax.broadcasted_iota(jnp.int32, (128, 128), 1)
    sub = lax.broadcasted_iota(jnp.int32, (128, 128), 0)
    table_s[...] = jnp.zeros((128, 128), F32)
    table_s[0:4, :] = routes_ref[...].astype(F32)
    table_s[4:8, :] = rweight_ref[...]
    tall = table_s[...].T
    hot = [(tall[:, k : k + 1] == lane.astype(F32)).astype(F32) for k in range(4)]
    every = (hot[0] + hot[1] + hot[2] + hot[3]).astype(BF16)
    before = jnp.dot((lane < sub).astype(BF16), every, preferred_element_type=F32)
    table = jnp.where(lane < 8, tall, 0.0)
    for k in range(4):
        rank = jnp.sum(hot[k] * before, axis=1, keepdims=True)
        table = jnp.where(lane == k, tall[:, k : k + 1] * 8.0 + rank, table)
    table = table.T[0:8, :]
    for d in range(3):
        meta[d, mine[d]] = table
    for d in range(3):
        for i in (1, 2, 3):
            ring_copy(meta.at[d], None, d, i, 0).start()

    def head_rows(h):
        return pl.ds(pl.multiple_of(h * TOK, TOK), TOK)

    def attend(slots, heads=(0, 1, 2, 3)):
        n = len(slots)
        width = n * TOK
        kt = jnp.concatenate([kt_all[s] for s in slots], axis=1)
        k2 = jnp.concatenate([kt, kt], axis=0)
        vv = jnp.concatenate([v_all[s] for s in slots], axis=0)
        v2 = jnp.concatenate([vv, jnp.ones_like(vv)], axis=1)

        def scores(h):
            return jnp.dot(q_hl[head_rows(h), :], k2, preferred_element_type=F32)

        s = scores(heads[0])
        for i, h in enumerate(heads):
            sl = head_rows(h)
            old = mstate[sl, :]
            top = s[:, 0:HD]
            for j in range(1, width // HD):
                top = jnp.maximum(top, s[:, j * HD : (j + 1) * HD])
            new = jnp.maximum(old, jnp.max(top, axis=1, keepdims=True))
            mstate[sl, :] = new
            p = jnp.exp2(s - new[:, 0:1]).astype(BF16)
            if i + 1 < len(heads):
                s = scores(heads[i + 1])
            shrink = jnp.exp2(old - new)
            pv = jnp.dot(p, v2, preferred_element_type=F32)
            acc[sl, :] = acc[sl, :] * jnp.concatenate([shrink, shrink], axis=1) + pv

    def pair_arrived(dy, dz, c):
        slot = origin(dy, dz, c)
        arrived(0, slot)
        arrived(1, slot)

    def to_sibling(group):
        for dy, dz in group:
            slot = origin(dy, dz, core)
            push(0, slot, sib)
            push(1, slot, sib)

    arrived(0, sib)
    arrived(1, sib)
    attend([sp, sib])

    for d in range(3):
        for i in (1, 2, 3):
            ring_arrived(meta.at[d], d, i, 0)

    def expert_of(d, q):
        if d == 0:
            return q * 4 + tx
        c, x = (q >> 2) & 1, q & 3
        if d == 1:
            return ((q >> 3) * 8 + yy * 2 + c) * 4 + x
        return (zz * 8 + (q >> 3) * 2 + c) * 4 + x

    def wanted(d, r):
        return (expert_of(d, r >> 4) * 8 + (r & 7) + ((r >> 3) & 1) * 4096).astype(F32)

    for d in range(3):
        want = wanted(d, lax.broadcasted_iota(jnp.int32, (512, 256), 0))
        for pair in range(2):
            first, second = meta[d, 2 * pair], meta[d, 2 * pair + 1]
            hit = None
            for k in range(4):
                have = jnp.concatenate(
                    [first[k : k + 1, :], second[k : k + 1, :] + 4096.0], axis=1
                )
                one = want == have
                hit = one if hit is None else hit | one
            place[d, pair] = jnp.where(hit, 1.0, 0.0).astype(BF16)
    for d in range(3):
        want = wanted(d, lax.broadcasted_iota(jnp.int32, (256, 512), 1))
        for pair in range(2):
            both = jnp.concatenate([meta[d, 2 * pair], meta[d, 2 * pair + 1]], axis=1)
            tall = jnp.concatenate([both, jnp.zeros((120, 256), F32)], axis=0).T
            shift = (lax.broadcasted_iota(jnp.int32, (256, 1), 0) >> 7).astype(F32) * 4096.0
            total = jnp.zeros((256, 512), F32)
            for k in range(4):
                total = jnp.where(
                    want == tall[:, k : k + 1] + shift, tall[:, 4 + k : 5 + k], total
                )
            total = total.astype(BF16)
            mixw[d, pair] = total

    def event(t):
        if t == 0:
            for dy, dz in A_SET:
                pair_arrived(dy, dz, core)
            turn = 1 + 2 * core
            for d in (1, 3):
                push(0, origin(d, 0, core), z_next)
                push(0, origin(d, 0, core), z_prev)
                push(1, origin(0, d, core), y_next)
                push(1, origin(0, d, core), y_prev)
            push(0, origin(turn, 0, core), at(yy + turn, zz, core))
            push(1, origin(0, turn, core), at(yy, zz + turn, core))
            push(0, origin(0, 1, core), z_next)
            push(1, origin(1, 0, core), y_next)
            to_sibling(A_SET)
        if t == 1:
            for dy, dz in A_SET:
                pair_arrived(dy, dz, 1 - core)
        if t == 2:
            for dy, dz in B_SET + C_SET:
                pair_arrived(dy, dz, core)
            push(0, origin(2, 0, core), z_next)
            push(0, origin(2, 0, core), z_prev)
            push(1, origin(0, 2, core), y_next)
            push(1, origin(0, 2, core), y_prev)
            push(0, origin(1, 1, core), z_next)
            push(0, origin(3, 3, core), z_prev)
            push(1, origin(1, 1, core), y_next)
            push(1, origin(3, 3, core), y_prev)
            to_sibling(B_SET + C_SET)
        if t == 3:
            for dy, dz in B_SET:
                pair_arrived(dy, dz, 1 - core)
        if t == 4:
            for dy, dz in D_SET:
                pair_arrived(dy, dz, core)
            push(0, origin(2, 3, core), z_prev)
            push(1, origin(3, 2, core), y_prev)
            to_sibling(D_SET)
            for dy, dz in C_SET:
                pair_arrived(dy, dz, 1 - core)
        if t == 5:
            pair_arrived(2, 2, core)
            to_sibling(E_SET)
        if t == 6:
            for dy, dz in D_SET:
                pair_arrived(dy, dz, 1 - core)

    groups = (
        [(dy, dz, 0) for dy, dz in A_SET],
        [(dy, dz, 1) for dy, dz in A_SET],
        [(dy, dz, 0) for dy, dz in B_SET],
        [(dy, dz, 1) for dy, dz in B_SET],
        [(2, 0, 0), (0, 2, 0), (2, 0, 1), (0, 2, 1)],
        [(dy, dz, 0) for dy, dz in D_SET],
        [(dy, dz, 1) for dy, dz in D_SET],
    )

    def chosen(values, t):
        code = sum(v * 4**i for i, v in enumerate(values))
        out = (code >> (2 * t)) % 4
        return out

    def one_step(t, carry):
        for i in range(7):

            @pl.when(t == i)
            def _(i=i):
                event(i)

        slots = []
        for j in range(4):
            dy = chosen([g[j][0] for g in groups], t)
            dz = chosen([g[j][1] for g in groups], t)
            flip = chosen([g[j][2] for g in groups], t)
            slots.append(origin(dy, dz, (core + flip) % 2))
        attend(slots)
        return carry

    lax.fori_loop(0, 6, one_step, 0)
    event(6)
    pair_arrived(2, 2, 1 - core)
    late = [origin(dy, dz, 1 - core) for dy, dz in D_SET]
    last = [origin(2, 2, core), origin(2, 2, 1 - core)]

    def head_copy(step, h, source):
        peer = (tx + step) % 4
        return pltpu.make_async_remote_copy(
            src_ref=o_tok.at[peer, h],
            dst_ref=hx_ref.at[source, h],
            send_sem=head_send.at[step, h],
            recv_sem=head_recv.at[source, h],
            device_id=(sp, peer),
            device_id_type=MESH,
        )

    def finish(pair, carry):
        heads = (2 * pair, 2 * pair + 1)
        attend(late, heads)
        attend(last, heads)
        for h in heads:
            a = acc[head_rows(h), :]
            o = (a[:, 0:HD] / a[:, HD : 2 * HD]).astype(BF16)
            for j in range(4):
                o_tok[j, h] = o[j * 128 : (j + 1) * 128, :]
            for step in (1, 2, 3):
                head_copy(step, h, tx).start()
            hx_ref[tx, h] = o_tok[tx, h]
        return carry

    lax.fori_loop(0, 2, finish, 0)
    loads[0].wait()
    for load in loads[7:]:
        load.wait()
    def project(d, pair):
        lo, hi = COLS[d]
        parts = []
        for j in range(4):
            buf = (back[d], sending[d])[j // 2]
            first = (j % 2) * 16 + pair * 8
            parts.append(buf[first : first + 8].reshape(256, hi - lo))
        weight = jnp.concatenate(parts, axis=0)
        some = [hx_ref[j, 2 * pair + h] for j in range(4) for h in range(2)]
        return jnp.dot(jnp.concatenate(some, axis=1), weight, preferred_element_type=F32)

    square = jnp.zeros((128, 128), F32)
    for pair in range(2):
        for h in (2 * pair, 2 * pair + 1):
            for step in (1, 2, 3):
                head_copy(step, h, (tx + step) % 4).wait_recv()
        for d in range(3):
            lo, hi = COLS[d]
            if pair == 0:
                shared[:, lo:hi] = project(d, 0)
                continue
            part = shared[:, lo:hi] + project(d, 1)
            h1 = (residual[:, lo:hi].astype(F32) + part).astype(BF16)
            hidden[:, lo:hi] = h1
            hf = h1.astype(F32)
            hf = hf * hf
            for j in range((hi - lo) // 128):
                square = square + hf[:, j * 128 : (j + 1) * 128]
    scale = lax.rsqrt(jnp.sum(square, axis=1, keepdims=True) * (1.0 / 2048.0) + EPS)
    for d in range(3):
        lo, hi = COLS[d]
        near[d][mine[d]] = (hidden[:, lo:hi].astype(F32) * scale * ng_ref[:, lo:hi]).astype(BF16)
        for i in (1, 2, 3):
            ring_copy(near[d], None, d, i, 1).start()

    def plane_copy(d, q, i, phase):
        return pltpu.make_async_remote_copy(
            src_ref=sending[d].at[q],
            dst_ref=(got, back)[phase][d].at[place_of[d]],
            send_sem=plane_send.at[phase, d, i],
            recv_sem=plane_recv.at[phase, d, place_of[d]],
            device_id=plane_device(d, q),
            device_id_type=MESH,
        )

    def spray(group, phase):
        for i, (da, db, dc) in enumerate(GROUPED):
            if da != group:
                continue
            c = (core + dc) % 2
            plane_copy(0, ((zz + da) % 4) * 8 + ((yy + db) % 4) * 2 + c, i, phase).start()
            plane_copy(1, ((zz + da) % 4) * 8 + c * 4 + (tx + db) % 4, i, phase).start()
            plane_copy(2, ((yy + da) % 4) * 8 + c * 4 + (tx + db) % 4, i, phase).start()

    def sprayed(phase):
        for d in range(3):

            def go(i, carry, d=d):
                plane_copy(d, (place_of[d] + 1) % 32, i, phase).wait_send()
                return carry

            lax.fori_loop(0, 31, go, 0)

    def plane_arrived(d, q, phase):
        buf = (got, back)[phase][d]
        pltpu.make_async_remote_copy(
            src_ref=buf.at[q],
            dst_ref=buf.at[q],
            send_sem=plane_send.at[phase, d, 0],
            recv_sem=plane_recv.at[phase, d, q],
            device_id=plane_device(d, (place_of[d] + 1) % 32),
            device_id_type=MESH,
        ).wait_recv()

    def each(lo, hi, act):
        def go(i, carry):
            act(i)
            return carry

        lax.fori_loop(lo, hi, go, 0)

    for d in range(3):
        for i in (1, 2, 3):
            ring_arrived(near[d], d, i, 1)
    for step in (2, 1, 3, 0):
        for d in range(3):
            width = COLS[d][1] - COLS[d][0]
            g = ((zz, zz, yy)[d] + step) % 4
            for pair in range(2):
                rows = near[d][2 * pair : 2 * pair + 2].reshape(256, width)
                pick = place[d, pair, pl.ds(pl.multiple_of(g * 128, 128), 128), :]
                moved = jnp.dot(pick, rows, preferred_element_type=F32).astype(BF16)
                sending[d][pl.ds(g * 8, 8), pair * 16 : (pair + 1) * 16, :] = moved.reshape(
                    8, 16, width
                )
        spray(step, 0)
    for d in range(3):
        got[d][place_of[d]] = sending[d][place_of[d]]

    for load in loads[1:7]:
        load.wait()
    gpart = jnp.zeros((128, 256), F32)
    upart = jnp.zeros((128, 256), F32)
    for d in range(3):
        lo, hi = COLS[d]
        rows = near[d][mine[d]]
        gpart = gpart + jnp.dot(rows, sgate[lo:hi, :], preferred_element_type=F32)
        upart = upart + jnp.dot(rows, sup[lo:hi, :], preferred_element_type=F32)
    shid = (jax.nn.silu(gpart) * upart).astype(BF16)
    for cb in range(4):
        sl = slice(cb * 512, (cb + 1) * 512)
        shared[:, sl] = jnp.dot(shid, sdown[:, sl], preferred_element_type=F32)

    def block_of(d, g, qi, j):
        if d == 0:
            return g * 32 + qi * 4 + j
        c, x = qi // 4, qi % 4
        if d == 1:
            return g * 32 + j * 8 + c * 4 + x
        return j * 32 + g * 8 + c * 4 + x

    for step in (2, 1, 3, 0):
        for d in range(3):
            lo, hi = COLS[d]
            g = ((zz, zz, yy)[d] + step) % 4
            if step:
                each(0, 8, lambda q, d=d, g=g: plane_arrived(d, g * 8 + q, 0))
            else:
                own = place_of[d] % 8
                each(
                    1,
                    8,
                    lambda q, d=d, g=g, own=own: plane_arrived(d, g * 8 + (own + q) % 8, 0),
                )
            rows = got[d][pl.ds(g * 8, 8)].reshape(256, hi - lo)
            for n, weight in enumerate((gate, up)):
                part = jnp.dot(rows, weight[lo:hi, :], preferred_element_type=F32)
                for qi in range(8):
                    for j in range(4):
                        at_row = (qi * 4 + j) * 8
                        b = block_of(d, g, qi, j)
                        piece = part[at_row : at_row + 8, :]
                        if d == 0:
                            gsum[0, n, b] = piece
                        elif d == 1:
                            gsum[0, n, b] = gsum[0, n, b] + piece
                        else:
                            gsum[1, n, b] = piece
    for z in range(4):
        sl = slice(z * 32, (z + 1) * 32)
        gg = (gsum[0, 0, sl] + gsum[1, 0, sl]).reshape(256, 256)
        uu = (gsum[0, 1, sl] + gsum[1, 1, sl]).reshape(256, 256)
        hsum[sl] = (jax.nn.silu(gg) * uu).reshape(32, 8, 256)
    sprayed(0)
    for step in (2, 1, 3, 0):
        for d in range(3):
            lo, hi = COLS[d]
            g = ((zz, zz, yy)[d] + step) % 4
            rows = jnp.concatenate(
                [hsum[block_of(d, g, qi, j)] for qi in range(8) for j in range(4)], axis=0
            ).astype(BF16)
            result = jnp.dot(rows, down[:, lo:hi], preferred_element_type=F32).astype(BF16)
            sending[d][pl.ds(g * 8, 8)] = result.reshape(8, 32, hi - lo)
        spray(step, 1)
    for d in range(3):
        back[d][place_of[d]] = sending[d][place_of[d]]
    for h in range(4):
        for step in (1, 2, 3):
            head_copy(step, h, tx).wait_send()
    for kind, index in sent:
        buf, recv = (kt_all, krecv) if kind == 0 else (v_all, vrecv)
        pltpu.make_async_remote_copy(
            src_ref=buf.at[sp],
            dst_ref=buf.at[sp],
            send_sem=send_sem.at[index],
            recv_sem=recv.at[sp],
            device_id=(sib, tx),
            device_id_type=MESH,
        ).wait_send()

    for d in range(3):
        for i in (1, 2, 3):
            ring_copy(near[d], None, d, i, 1).wait_send()
            ring_copy(meta.at[d], None, d, i, 0).wait_send()
    for d in range(3):
        lo, hi = COLS[d]
        width = hi - lo
        each(1, 32, lambda q, d=d: plane_arrived(d, (place_of[d] + q) % 32, 1))
        for pair in range(2):
            rows = back[d][:, pair * 16 : (pair + 1) * 16, :].reshape(512, width)
            part = jnp.dot(mixw[d, pair], rows, preferred_element_type=F32).astype(BF16)
            near[d][2 * pair : 2 * pair + 2] = part.reshape(2, 128, width)
        for i in (1, 2, 3):
            ring_copy(near[d], fin[d], d, i, 2).start()
        fin[d][mine[d]] = near[d][mine[d]]
    for d in range(3):
        lo, hi = COLS[d]
        for i in (1, 2, 3):
            ring_arrived(fin[d], d, i, 2)
        total = hidden[:, lo:hi].astype(F32) + shared[:, lo:hi]
        for j in range(4):
            total = total + fin[d][j].astype(F32)
        out_ref[:, lo:hi] = total.astype(BF16)
    for d in range(3):
        for i in (1, 2, 3):
            ring_copy(near[d], fin[d], d, i, 2).wait_send()
    sprayed(1)


def layer(*operands):
    rows, cols = rotary_tables()
    vmem = pl.BlockSpec(memory_space=pltpu.VMEM)
    hbm = pl.BlockSpec(memory_space=pl.ANY)
    widths = [hi - lo for lo, hi in COLS]
    weight = pltpu.VMEM((2048, 256), BF16)
    return pl.pallas_call(
        layer_kernel,
        out_shape=jax.ShapeDtypeStruct((128, 2048), BF16),
        in_specs=[hbm] * 18,
        out_specs=vmem,
        scratch_shapes=[
            pltpu.VMEM((TOK, 4 * HD), BF16),
            pltpu.VMEM((TOK, HD), BF16),
            pltpu.VMEM((1, HD), F32),
            pltpu.VMEM((1, HD), F32),
            pltpu.VMEM((2, 8, HD), F32),
            pltpu.VMEM((2, GRID_W, HD), F32),
            pltpu.VMEM((1, 2048), F32),
            pltpu.VMEM((4, 128), jnp.int32),
            pltpu.VMEM((4, 128), F32),
            pltpu.VMEM((4, 4, 128, HD), BF16),
            pltpu.VMEM((32, HD, TOK), BF16),
            pltpu.VMEM((32, TOK, HD), BF16),
            pltpu.VMEM((4 * TOK, 2 * HD), BF16),
            pltpu.VMEM((2, TOK, HD), F32),
            pltpu.VMEM((4 * TOK, 2 * HD), F32),
            pltpu.VMEM((4 * TOK, HD), F32),
            pltpu.VMEM((4, 4, 128, HD), BF16),
            pltpu.VMEM((128, 2048), BF16),
            weight,
            weight,
            pltpu.VMEM((256, 2048), BF16),
            weight,
            weight,
            pltpu.VMEM((256, 2048), BF16),
            pltpu.VMEM((128, 2048), BF16),
            pltpu.VMEM((128, 2048), F32),
            pltpu.VMEM((3, 4, 8, 128), F32),
            pltpu.VMEM((128, 128), F32),
            pltpu.VMEM((3, 2, 512, 256), BF16),
            pltpu.VMEM((3, 2, 256, 512), BF16),
        ]
        + [pltpu.VMEM((4, 128, w), BF16) for w in widths]
        + [pltpu.VMEM((32, 32, w), BF16) for w in widths * 3]
        + [pltpu.VMEM((4, 128, w), BF16) for w in widths]
        + [
            pltpu.VMEM((2, 2, 128, 8, 256), F32),
            pltpu.VMEM((128, 8, 256), F32),
            pltpu.SemaphoreType.DMA((72,)),
            pltpu.SemaphoreType.DMA((32,)),
            pltpu.SemaphoreType.DMA((32,)),
            pltpu.SemaphoreType.DMA((4, 4)),
            pltpu.SemaphoreType.DMA((4, 4)),
            pltpu.SemaphoreType.DMA((13,)),
            pltpu.SemaphoreType.DMA((10,)),
            pltpu.SemaphoreType.DMA((3, 3, 4)),
            pltpu.SemaphoreType.DMA((3, 3, 4)),
            pltpu.SemaphoreType.DMA((2, 3, 32)),
            pltpu.SemaphoreType.DMA((2, 3, 32)),
        ],
        compiler_params=pltpu.CompilerParams(
            collective_id=0, has_side_effects=True, vmem_limit_bytes=67043328
        ),
        name="layer",
    )(*operands[:5], jnp.asarray(rows), jnp.asarray(cols), *operands[5:])


def body(
    queries,
    keys,
    values,
    residual,
    out_proj,
    query_gain,
    key_gain,
    norm_gain,
    routes,
    route_weight,
    expert_gate,
    expert_up,
    expert_down,
    shared_gate,
    shared_up,
    shared_down,
):
    return layer(
        queries,
        keys,
        values,
        query_gain.reshape(1, HD),
        key_gain.reshape(1, HD),
        norm_gain.reshape(1, 2048),
        routes.T,
        route_weight.T,
        residual,
        out_proj.reshape(64, 32, 2048),
        expert_gate,
        expert_up,
        expert_down,
        shared_gate,
        shared_up,
        shared_down,
    )


def solution(mesh):
    placed = (
        P("sp", "tp"),
        P("sp", "tp"),
        P("sp", "tp"),
        P(("sp", "tp"), None),
        P(),
        P(),
        P(),
        P(),
        P(("sp", "tp"), None),
        P(("sp", "tp"), None),
        P(("sp", "tp"), None, None),
        P(("sp", "tp"), None, None),
        P(("sp", "tp"), None, None),
        P(),
        P(),
        P(),
    )
    return jax.shard_map(
        body, mesh=mesh, in_specs=placed, out_specs=P(("sp", "tp"), None), check_vma=False
    )
```

```python
import math

import jax
import jax.numpy as jnp
import numpy as np
from jax import lax
from jax.experimental import pallas as pl
from jax.experimental.pallas import tpu as pltpu
from jax.sharding import PartitionSpec as P

HEADS = 16
KV_HEADS = 4
GRID_W = 64
HD = 128
TOK = 512
EPS = 1e-06
THETA = 10000.0
MESH = pl.DeviceIdType.MESH
F32 = jnp.float32
BF16 = jnp.bfloat16


def rotary_tables():
    quarter = HD // 4
    inverse = (THETA ** (-4.0 * np.arange(quarter, dtype=np.float64) / HD)).astype(np.float32)

    def table(count):
        angle = np.arange(count, dtype=np.float32)[:, None] * inverse[None, :]
        angle = angle.astype(np.float32).astype(np.float64)
        cosine = np.cos(angle).astype(np.float32)
        sine = np.sin(angle).astype(np.float32)
        return np.concatenate([cosine, cosine], 1), np.concatenate([-sine, sine], 1)

    row_cos, row_sin = table(256)
    col_cos, col_sin = table(GRID_W)
    zr, zc = np.zeros_like(row_cos), np.zeros_like(col_cos)
    rows = np.stack([np.concatenate([row_cos, zr], 1), np.concatenate([row_sin, zr], 1)])
    cols = np.stack([np.concatenate([zc, col_cos], 1), np.concatenate([zc, col_sin], 1)])
    return rows, cols


def normed_rotary(source, gain, cos_t, sin_t):
    x = source.astype(F32)
    x = x * lax.rsqrt(jnp.mean(x * x, axis=-1, keepdims=True) + EPS) * gain
    lane = lax.broadcasted_iota(jnp.int32, x.shape, 1)
    partner = jnp.where((lane // 32) % 2 == 0, pltpu.roll(x, 96, 1), pltpu.roll(x, 32, 1))
    return x * cos_t + partner * sin_t


A_SET = ((1, 0), (3, 0), (0, 1), (0, 3))
B_SET = ((1, 1), (1, 3), (3, 1), (3, 3))
C_SET = ((2, 0), (0, 2))
D_SET = ((2, 1), (2, 3), (1, 2), (3, 2))
E_SET = ((2, 2),)


def far(a):
    return 2 if a == 2 else a % 2


PLANE = [(a, b, c) for a in range(4) for b in range(4) for c in range(2) if a or b or c]
FARTHEST = sorted(PLANE, key=lambda m: -far(m[0]) - far(m[1]))
GROUPED = sorted(PLANE, key=lambda m: (-far(m[0]), -far(m[1]), m[2], m[1], m[0]))
COLS = ((0, 640), (640, 1280), (1280, 2048))


def layer_kernel(
    q_ref,
    k_ref,
    v_ref,
    qg_ref,
    kg_ref,
    rows_ref,
    cols_ref,
    ng_ref,
    routes_ref,
    rweight_ref,
    residual_hbm,
    out_proj_hbm,
    gate_hbm,
    up_hbm,
    down_hbm,
    sgate_hbm,
    sup_hbm,
    sdown_hbm,
    out_ref,
    hx_ref,
    kt_all,
    v_all,
    q_hl,
    trig,
    acc,
    mstate,
    o_tok,
    residual,
    gate,
    up,
    down,
    sgate,
    sup,
    sdown,
    hidden,
    shared,
    meta,
    table_s,
    place,
    mixw,
    nbx,
    nby,
    nbz,
    sendx,
    sendy,
    sendz,
    gotx,
    goty,
    gotz,
    backx,
    backy,
    backz,
    finx,
    finy,
    finz,
    gsum,
    hsum,
    send_sem,
    krecv,
    vrecv,
    head_send,
    head_recv,
    load_sem,
    ring_send,
    ring_recv,
    plane_send,
    plane_recv,
):
    near = (nbx, nby, nbz)
    sending = (sendx, sendy, sendz)
    got = (gotx, goty, gotz)
    back = (backx, backy, backz)
    fin = (finx, finy, finz)
    loads = [
        pltpu.make_async_copy(src, dst, load_sem.at[i])
        for i, (src, dst) in enumerate(
            (
                (residual_hbm, residual),
                (gate_hbm.at[0], gate),
                (up_hbm.at[0], up),
                (down_hbm.at[0], down),
                (sgate_hbm, sgate),
                (sup_hbm, sup),
                (sdown_hbm, sdown),
            )
        )
    ]
    for d, (lo, hi) in enumerate(COLS):
        for half, dst in enumerate((back[d], sending[d])):
            src = out_proj_hbm.at[pl.ds(half * 32, 32), :, lo:hi]
            loads.append(pltpu.make_async_copy(src, dst, load_sem.at[7 + 2 * d + half]))
    sp = lax.axis_index("sp")
    tx = lax.axis_index("tp")
    core = sp % 2
    yy = (sp // 2) % 4
    zz = sp // 8

    def at(y, z, c):
        return (z % 4) * 8 + (y % 4) * 2 + c

    sib = at(yy, zz, 1 - core)
    y_next, y_prev = at(yy + 1, zz, core), at(yy + 3, zz, core)
    z_next, z_prev = at(yy, zz + 1, core), at(yy, zz + 3, core)

    mine = (tx, yy, zz)
    place_of = (sp, zz * 8 + core * 4 + tx, yy * 8 + core * 4 + tx)

    def plane_device(d, q):
        if d == 0:
            return (q, tx)
        c, x = (q // 4) % 2, q % 4
        if d == 1:
            return ((q // 8) * 8 + yy * 2 + c, x)
        return (zz * 8 + (q // 8) * 2 + c, x)

    def ring_device(d, j):
        if d == 0:
            return (sp, j)
        if d == 1:
            return (at(j, zz, core), tx)
        return (at(yy, j, core), tx)

    barrier = pltpu.get_barrier_semaphore()
    peers = [(sib, tx)] + [ring_device(d, (mine[d] + i) % 4) for d in range(3) for i in (1, 2, 3)]
    for peer in peers:
        pl.semaphore_signal(barrier, inc=1, device_id=peer, device_id_type=MESH)

    counter = [0]
    sent = []

    def push(kind, slot, peer):
        buf, recv = (kt_all, krecv) if kind == 0 else (v_all, vrecv)
        copy = pltpu.make_async_remote_copy(
            src_ref=buf.at[slot],
            dst_ref=buf.at[slot],
            send_sem=send_sem.at[counter[0]],
            recv_sem=recv.at[slot],
            device_id=(peer, tx),
            device_id_type=MESH,
        )
        sent.append((kind, counter[0]))
        counter[0] += 1
        copy.start()

    def arrived(kind, slot):
        buf, recv = (kt_all, krecv) if kind == 0 else (v_all, vrecv)
        pltpu.make_async_remote_copy(
            src_ref=buf.at[slot],
            dst_ref=buf.at[slot],
            send_sem=send_sem.at[0],
            recv_sem=recv.at[slot],
            device_id=(sib, tx),
            device_id_type=MESH,
        ).wait_recv()

    def origin(dy, dz, c):
        return at(yy - dy + 4, zz - dz + 4, c)

    for r in range(8):
        sl = pl.ds(r * GRID_W, GRID_W)
        for i in range(2):
            trig[i, sl, :] = rows_ref[i, pl.ds(sp * 8 + r, 1), :] + cols_ref[i]

    kr = normed_rotary(k_ref[...], kg_ref[...], trig[0], trig[1])
    kt_all[sp] = kr.T.astype(BF16)
    v_all[sp] = v_ref[...]
    factor = math.log2(math.e) / math.sqrt(HD)
    for h in range(4):
        qr = normed_rotary(q_ref[:, h * HD : (h + 1) * HD], qg_ref[...], trig[0], trig[1])
        qs = qr.astype(BF16).astype(F32) * factor
        hi = qs.astype(BF16)
        q_hl[h * TOK : (h + 1) * TOK, 0:HD] = hi
        q_hl[h * TOK : (h + 1) * TOK, HD : 2 * HD] = (qs - hi.astype(F32)).astype(BF16)
    acc[...] = jnp.zeros_like(acc)
    mstate[...] = jnp.full_like(mstate, -1e30)

    def ring_copy(buf, dst, d, i, phase):
        j = (mine[d] + i) % 4
        if dst is None:
            source, target = buf.at[mine[d]], buf.at[mine[d]]
        else:
            source, target = buf.at[j], dst.at[mine[d]]
        return pltpu.make_async_remote_copy(
            src_ref=source,
            dst_ref=target,
            send_sem=ring_send.at[phase, d, i],
            recv_sem=ring_recv.at[phase, d, mine[d]],
            device_id=ring_device(d, j),
            device_id_type=MESH,
        )

    def ring_arrived(buf, d, i, phase):
        j = (mine[d] + i) % 4
        pltpu.make_async_remote_copy(
            src_ref=buf.at[j],
            dst_ref=buf.at[j],
            send_sem=ring_send.at[phase, d, i],
            recv_sem=ring_recv.at[phase, d, j],
            device_id=ring_device(d, j),
            device_id_type=MESH,
        ).wait_recv()

    pl.semaphore_wait(barrier, 10)
    for kind in (0, 1):
        for peer in (y_next, y_prev, z_next, z_prev):
            push(kind, sp, peer)
    push(0, sp, sib)
    push(1, sp, sib)
    for load in loads:
        load.start()

    lane = lax.broadcasted_iota(jnp.int32, (128, 128), 1)
    sub = lax.broadcasted_iota(jnp.int32, (128, 128), 0)
    table_s[...] = jnp.zeros((128, 128), F32)
    table_s[0:4, :] = routes_ref[...].astype(F32)
    table_s[4:8, :] = rweight_ref[...]
    tall = table_s[...].T
    hot = [(tall[:, k : k + 1] == lane.astype(F32)).astype(F32) for k in range(4)]
    every = (hot[0] + hot[1] + hot[2] + hot[3]).astype(BF16)
    before = jnp.dot((lane < sub).astype(BF16), every, preferred_element_type=F32)
    table = jnp.where(lane < 8, tall, 0.0)
    for k in range(4):
        rank = jnp.sum(hot[k] * before, axis=1, keepdims=True)
        table = jnp.where(lane == k, tall[:, k : k + 1] * 8.0 + rank, table)
    table = table.T[0:8, :]
    for d in range(3):
        meta[d, mine[d]] = table
    for d in range(3):
        for i in (1, 2, 3):
            ring_copy(meta.at[d], None, d, i, 0).start()

    def head_rows(h):
        return pl.ds(pl.multiple_of(h * TOK, TOK), TOK)

    def attend(slots, heads=(0, 1, 2, 3)):
        n = len(slots)
        width = n * TOK
        kt = jnp.concatenate([kt_all[s] for s in slots], axis=1)
        k2 = jnp.concatenate([kt, kt], axis=0)
        vv = jnp.concatenate([v_all[s] for s in slots], axis=0)
        v2 = jnp.concatenate([vv, jnp.ones_like(vv)], axis=1)

        def scores(h):
            return jnp.dot(q_hl[head_rows(h), :], k2, preferred_element_type=F32)

        s = scores(heads[0])
        for i, h in enumerate(heads):
            sl = head_rows(h)
            old = mstate[sl, :]
            top = s[:, 0:HD]
            for j in range(1, width // HD):
                top = jnp.maximum(top, s[:, j * HD : (j + 1) * HD])
            new = jnp.maximum(old, jnp.max(top, axis=1, keepdims=True))
            mstate[sl, :] = new
            p = jnp.exp2(s - new[:, 0:1]).astype(BF16)
            if i + 1 < len(heads):
                s = scores(heads[i + 1])
            shrink = jnp.exp2(old - new)
            pv = jnp.dot(p, v2, preferred_element_type=F32)
            acc[sl, :] = acc[sl, :] * jnp.concatenate([shrink, shrink], axis=1) + pv

    def pair_arrived(dy, dz, c):
        slot = origin(dy, dz, c)
        arrived(0, slot)
        arrived(1, slot)

    def to_sibling(group):
        for dy, dz in group:
            slot = origin(dy, dz, core)
            push(0, slot, sib)
            push(1, slot, sib)

    arrived(0, sib)
    arrived(1, sib)
    attend([sp, sib])

    for d in range(3):
        for i in (1, 2, 3):
            ring_arrived(meta.at[d], d, i, 0)

    def expert_of(d, q):
        if d == 0:
            return q * 4 + tx
        c, x = (q >> 2) & 1, q & 3
        if d == 1:
            return ((q >> 3) * 8 + yy * 2 + c) * 4 + x
        return (zz * 8 + (q >> 3) * 2 + c) * 4 + x

    def wanted(d, r):
        return (expert_of(d, r >> 4) * 8 + (r & 7) + ((r >> 3) & 1) * 4096).astype(F32)

    for d in range(3):
        want = wanted(d, lax.broadcasted_iota(jnp.int32, (512, 256), 0))
        for pair in range(2):
            first, second = meta[d, 2 * pair], meta[d, 2 * pair + 1]
            hit = None
            for k in range(4):
                have = jnp.concatenate(
                    [first[k : k + 1, :], second[k : k + 1, :] + 4096.0], axis=1
                )
                one = want == have
                hit = one if hit is None else hit | one
            place[d, pair] = jnp.where(hit, 1.0, 0.0).astype(BF16)
    for d in range(3):
        want = wanted(d, lax.broadcasted_iota(jnp.int32, (256, 512), 1))
        for pair in range(2):
            both = jnp.concatenate([meta[d, 2 * pair], meta[d, 2 * pair + 1]], axis=1)
            tall = jnp.concatenate([both, jnp.zeros((120, 256), F32)], axis=0).T
            shift = (lax.broadcasted_iota(jnp.int32, (256, 1), 0) >> 7).astype(F32) * 4096.0
            total = jnp.zeros((256, 512), F32)
            for k in range(4):
                total = jnp.where(
                    want == tall[:, k : k + 1] + shift, tall[:, 4 + k : 5 + k], total
                )
            total = total.astype(BF16)
            mixw[d, pair] = total

    def event(t):
        if t == 0:
            for dy, dz in A_SET:
                pair_arrived(dy, dz, core)
            turn = 1 + 2 * core
            for d in (1, 3):
                push(0, origin(d, 0, core), z_next)
                push(0, origin(d, 0, core), z_prev)
                push(1, origin(0, d, core), y_next)
                push(1, origin(0, d, core), y_prev)
            push(0, origin(turn, 0, core), at(yy + turn, zz, core))
            push(1, origin(0, turn, core), at(yy, zz + turn, core))
            push(0, origin(0, 1, core), z_next)
            push(1, origin(1, 0, core), y_next)
            to_sibling(A_SET)
        if t == 1:
            for dy, dz in A_SET:
                pair_arrived(dy, dz, 1 - core)
        if t == 2:
            for dy, dz in B_SET + C_SET:
                pair_arrived(dy, dz, core)
            push(0, origin(2, 0, core), z_next)
            push(0, origin(2, 0, core), z_prev)
            push(1, origin(0, 2, core), y_next)
            push(1, origin(0, 2, core), y_prev)
            push(0, origin(1, 1, core), z_next)
            push(0, origin(3, 3, core), z_prev)
            push(1, origin(1, 1, core), y_next)
            push(1, origin(3, 3, core), y_prev)
            to_sibling(B_SET + C_SET)
        if t == 3:
            for dy, dz in B_SET:
                pair_arrived(dy, dz, 1 - core)
        if t == 4:
            for dy, dz in D_SET:
                pair_arrived(dy, dz, core)
            push(0, origin(2, 3, core), z_prev)
            push(1, origin(3, 2, core), y_prev)
            to_sibling(D_SET)
            for dy, dz in C_SET:
                pair_arrived(dy, dz, 1 - core)
        if t == 5:
            pair_arrived(2, 2, core)
            to_sibling(E_SET)
        if t == 6:
            for dy, dz in D_SET:
                pair_arrived(dy, dz, 1 - core)

    groups = (
        [(dy, dz, 0) for dy, dz in A_SET],
        [(dy, dz, 1) for dy, dz in A_SET],
        [(dy, dz, 0) for dy, dz in B_SET],
        [(dy, dz, 1) for dy, dz in B_SET],
        [(2, 0, 0), (0, 2, 0), (2, 0, 1), (0, 2, 1)],
        [(dy, dz, 0) for dy, dz in D_SET],
        [(dy, dz, 1) for dy, dz in D_SET],
    )

    def chosen(values, t):
        code = sum(v * 4**i for i, v in enumerate(values))
        out = (code >> (2 * t)) % 4
        return out

    def one_step(t, carry):
        for i in range(7):

            @pl.when(t == i)
            def _(i=i):
                event(i)

        slots = []
        for j in range(4):
            dy = chosen([g[j][0] for g in groups], t)
            dz = chosen([g[j][1] for g in groups], t)
            flip = chosen([g[j][2] for g in groups], t)
            slots.append(origin(dy, dz, (core + flip) % 2))
        attend(slots)
        return carry

    lax.fori_loop(0, 6, one_step, 0)
    event(6)
    pair_arrived(2, 2, 1 - core)
    late = [origin(dy, dz, 1 - core) for dy, dz in D_SET]
    last = [origin(2, 2, core), origin(2, 2, 1 - core)]

    def head_copy(step, h, source):
        peer = (tx + step) % 4
        return pltpu.make_async_remote_copy(
            src_ref=o_tok.at[peer, h],
            dst_ref=hx_ref.at[source, h],
            send_sem=head_send.at[step, h],
            recv_sem=head_recv.at[source, h],
            device_id=(sp, peer),
            device_id_type=MESH,
        )

    def finish(pair, carry):
        heads = (2 * pair, 2 * pair + 1)
        attend(late, heads)
        attend(last, heads)
        for h in heads:
            a = acc[head_rows(h), :]
            o = (a[:, 0:HD] / a[:, HD : 2 * HD]).astype(BF16)
            for j in range(4):
                o_tok[j, h] = o[j * 128 : (j + 1) * 128, :]
            for step in (1, 2, 3):
                head_copy(step, h, tx).start()
            hx_ref[tx, h] = o_tok[tx, h]
        return carry

    lax.fori_loop(0, 2, finish, 0)
    loads[0].wait()
    for load in loads[7:]:
        load.wait()
    def project(d, pair):
        lo, hi = COLS[d]
        parts = []
        for j in range(4):
            buf = (back[d], sending[d])[j // 2]
            first = (j % 2) * 16 + pair * 8
            parts.append(buf[first : first + 8].reshape(256, hi - lo))
        weight = jnp.concatenate(parts, axis=0)
        some = [hx_ref[j, 2 * pair + h] for j in range(4) for h in range(2)]
        return jnp.dot(jnp.concatenate(some, axis=1), weight, preferred_element_type=F32)

    square = jnp.zeros((128, 128), F32)
    for pair in range(2):
        for h in (2 * pair, 2 * pair + 1):
            for step in (1, 2, 3):
                head_copy(step, h, (tx + step) % 4).wait_recv()
        for d in range(3):
            lo, hi = COLS[d]
            if pair == 0:
                shared[:, lo:hi] = project(d, 0)
                continue
            part = shared[:, lo:hi] + project(d, 1)
            h1 = (residual[:, lo:hi].astype(F32) + part).astype(BF16)
            hidden[:, lo:hi] = h1
            hf = h1.astype(F32)
            hf = hf * hf
            for j in range((hi - lo) // 128):
                square = square + hf[:, j * 128 : (j + 1) * 128]
    scale = lax.rsqrt(jnp.sum(square, axis=1, keepdims=True) * (1.0 / 2048.0) + EPS)
    for d in range(3):
        lo, hi = COLS[d]
        near[d][mine[d]] = (hidden[:, lo:hi].astype(F32) * scale * ng_ref[:, lo:hi]).astype(BF16)
        for i in (1, 2, 3):
            ring_copy(near[d], None, d, i, 1).start()

    def plane_copy(d, q, i, phase):
        return pltpu.make_async_remote_copy(
            src_ref=sending[d].at[q],
            dst_ref=(got, back)[phase][d].at[place_of[d]],
            send_sem=plane_send.at[phase, d, i],
            recv_sem=plane_recv.at[phase, d, place_of[d]],
            device_id=plane_device(d, q),
            device_id_type=MESH,
        )

    def spray(order, phase):
        for i, (da, db, dc) in enumerate(order):
            c = (core + dc) % 2
            plane_copy(0, ((zz + da) % 4) * 8 + ((yy + db) % 4) * 2 + c, i, phase).start()
            plane_copy(1, ((zz + da) % 4) * 8 + c * 4 + (tx + db) % 4, i, phase).start()
            plane_copy(2, ((yy + da) % 4) * 8 + c * 4 + (tx + db) % 4, i, phase).start()

    def sprayed(phase):
        for d in range(3):

            def go(i, carry, d=d):
                plane_copy(d, (place_of[d] + 1) % 32, i, phase).wait_send()
                return carry

            lax.fori_loop(0, 31, go, 0)

    def plane_arrived(d, q, phase):
        buf = (got, back)[phase][d]
        pltpu.make_async_remote_copy(
            src_ref=buf.at[q],
            dst_ref=buf.at[q],
            send_sem=plane_send.at[phase, d, 0],
            recv_sem=plane_recv.at[phase, d, q],
            device_id=plane_device(d, (place_of[d] + 1) % 32),
            device_id_type=MESH,
        ).wait_recv()

    def each(lo, hi, act):
        def go(i, carry):
            act(i)
            return carry

        lax.fori_loop(lo, hi, go, 0)

    for d in range(3):
        width = COLS[d][1] - COLS[d][0]
        for i in (1, 2, 3):
            ring_arrived(near[d], d, i, 1)
        for pair in range(2):
            rows = near[d][2 * pair : 2 * pair + 2].reshape(256, width)
            moved = jnp.dot(place[d, pair], rows, preferred_element_type=F32).astype(BF16)
            sending[d][:, pair * 16 : (pair + 1) * 16, :] = moved.reshape(32, 16, width)
        got[d][place_of[d]] = sending[d][place_of[d]]
    spray(GROUPED, 0)

    for h in range(4):
        for step in (1, 2, 3):
            head_copy(step, h, tx).wait_send()
    for kind, index in sent:
        buf, recv = (kt_all, krecv) if kind == 0 else (v_all, vrecv)
        pltpu.make_async_remote_copy(
            src_ref=buf.at[sp],
            dst_ref=buf.at[sp],
            send_sem=send_sem.at[index],
            recv_sem=recv.at[sp],
            device_id=(sib, tx),
            device_id_type=MESH,
        ).wait_send()
    for load in loads[1:7]:
        load.wait()
    gpart = jnp.zeros((128, 256), F32)
    upart = jnp.zeros((128, 256), F32)
    for d in range(3):
        lo, hi = COLS[d]
        rows = near[d][mine[d]]
        gpart = gpart + jnp.dot(rows, sgate[lo:hi, :], preferred_element_type=F32)
        upart = upart + jnp.dot(rows, sup[lo:hi, :], preferred_element_type=F32)
    shid = (jax.nn.silu(gpart) * upart).astype(BF16)
    for cb in range(4):
        sl = slice(cb * 512, (cb + 1) * 512)
        shared[:, sl] = jnp.dot(shid, sdown[:, sl], preferred_element_type=F32)

    def block_of(d, g, qi, j):
        if d == 0:
            return g * 32 + qi * 4 + j
        c, x = qi // 4, qi % 4
        if d == 1:
            return g * 32 + j * 8 + c * 4 + x
        return j * 32 + g * 8 + c * 4 + x

    for step in (2, 1, 3, 0):
        for d in range(3):
            lo, hi = COLS[d]
            g = ((zz, zz, yy)[d] + step) % 4
            if step:
                each(0, 8, lambda q, d=d, g=g: plane_arrived(d, g * 8 + q, 0))
            else:
                own = place_of[d] % 8
                each(
                    1,
                    8,
                    lambda q, d=d, g=g, own=own: plane_arrived(d, g * 8 + (own + q) % 8, 0),
                )
            rows = got[d][pl.ds(g * 8, 8)].reshape(256, hi - lo)
            for n, weight in enumerate((gate, up)):
                part = jnp.dot(rows, weight[lo:hi, :], preferred_element_type=F32)
                for qi in range(8):
                    for j in range(4):
                        at_row = (qi * 4 + j) * 8
                        b = block_of(d, g, qi, j)
                        piece = part[at_row : at_row + 8, :]
                        if d == 0:
                            gsum[0, n, b] = piece
                        elif d == 1:
                            gsum[0, n, b] = gsum[0, n, b] + piece
                        else:
                            gsum[1, n, b] = piece
    for z in range(4):
        sl = slice(z * 32, (z + 1) * 32)
        gg = (gsum[0, 0, sl] + gsum[1, 0, sl]).reshape(256, 256)
        uu = (gsum[0, 1, sl] + gsum[1, 1, sl]).reshape(256, 256)
        hsum[sl] = (jax.nn.silu(gg) * uu).reshape(32, 8, 256)
    sprayed(0)
    for d in range(3):
        lo, hi = COLS[d]
        for g in range(4):
            rows = jnp.concatenate(
                [hsum[block_of(d, g, qi, j)] for qi in range(8) for j in range(4)], axis=0
            ).astype(BF16)
            result = jnp.dot(rows, down[:, lo:hi], preferred_element_type=F32).astype(BF16)
            sending[d][g * 8 : g * 8 + 8] = result.reshape(8, 32, hi - lo)
        back[d][place_of[d]] = sending[d][place_of[d]]
    spray(FARTHEST, 1)

    for d in range(3):
        for i in (1, 2, 3):
            ring_copy(near[d], None, d, i, 1).wait_send()
            ring_copy(meta.at[d], None, d, i, 0).wait_send()
    for d in range(3):
        lo, hi = COLS[d]
        width = hi - lo
        each(1, 32, lambda q, d=d: plane_arrived(d, (place_of[d] + q) % 32, 1))
        for pair in range(2):
            rows = back[d][:, pair * 16 : (pair + 1) * 16, :].reshape(512, width)
            part = jnp.dot(mixw[d, pair], rows, preferred_element_type=F32).astype(BF16)
            near[d][2 * pair : 2 * pair + 2] = part.reshape(2, 128, width)
        for i in (1, 2, 3):
            ring_copy(near[d], fin[d], d, i, 2).start()
        fin[d][mine[d]] = near[d][mine[d]]
    for d in range(3):
        lo, hi = COLS[d]
        for i in (1, 2, 3):
            ring_arrived(fin[d], d, i, 2)
        total = hidden[:, lo:hi].astype(F32) + shared[:, lo:hi]
        for j in range(4):
            total = total + fin[d][j].astype(F32)
        out_ref[:, lo:hi] = total.astype(BF16)
    for d in range(3):
        for i in (1, 2, 3):
            ring_copy(near[d], fin[d], d, i, 2).wait_send()
    sprayed(1)


def layer(*operands):
    rows, cols = rotary_tables()
    vmem = pl.BlockSpec(memory_space=pltpu.VMEM)
    hbm = pl.BlockSpec(memory_space=pl.ANY)
    widths = [hi - lo for lo, hi in COLS]
    weight = pltpu.VMEM((2048, 256), BF16)
    return pl.pallas_call(
        layer_kernel,
        out_shape=jax.ShapeDtypeStruct((128, 2048), BF16),
        in_specs=[vmem] * 10 + [hbm] * 8,
        out_specs=vmem,
        scratch_shapes=[
            pltpu.VMEM((4, 4, 128, HD), BF16),
            pltpu.VMEM((32, HD, TOK), BF16),
            pltpu.VMEM((32, TOK, HD), BF16),
            pltpu.VMEM((4 * TOK, 2 * HD), BF16),
            pltpu.VMEM((2, TOK, HD), F32),
            pltpu.VMEM((4 * TOK, 2 * HD), F32),
            pltpu.VMEM((4 * TOK, HD), F32),
            pltpu.VMEM((4, 4, 128, HD), BF16),
            pltpu.VMEM((128, 2048), BF16),
            weight,
            weight,
            pltpu.VMEM((256, 2048), BF16),
            weight,
            weight,
            pltpu.VMEM((256, 2048), BF16),
            pltpu.VMEM((128, 2048), BF16),
            pltpu.VMEM((128, 2048), F32),
            pltpu.VMEM((3, 4, 8, 128), F32),
            pltpu.VMEM((128, 128), F32),
            pltpu.VMEM((3, 2, 512, 256), BF16),
            pltpu.VMEM((3, 2, 256, 512), BF16),
        ]
        + [pltpu.VMEM((4, 128, w), BF16) for w in widths]
        + [pltpu.VMEM((32, 32, w), BF16) for w in widths * 3]
        + [pltpu.VMEM((4, 128, w), BF16) for w in widths]
        + [
            pltpu.VMEM((2, 2, 128, 8, 256), F32),
            pltpu.VMEM((128, 8, 256), F32),
            pltpu.SemaphoreType.DMA((72,)),
            pltpu.SemaphoreType.DMA((32,)),
            pltpu.SemaphoreType.DMA((32,)),
            pltpu.SemaphoreType.DMA((4, 4)),
            pltpu.SemaphoreType.DMA((4, 4)),
            pltpu.SemaphoreType.DMA((13,)),
            pltpu.SemaphoreType.DMA((3, 3, 4)),
            pltpu.SemaphoreType.DMA((3, 3, 4)),
            pltpu.SemaphoreType.DMA((2, 3, 32)),
            pltpu.SemaphoreType.DMA((2, 3, 32)),
        ],
        compiler_params=pltpu.CompilerParams(
            collective_id=0, has_side_effects=True, vmem_limit_bytes=67043328
        ),
        name="layer",
    )(*operands[:5], jnp.asarray(rows), jnp.asarray(cols), *operands[5:])


def body(
    queries,
    keys,
    values,
    residual,
    out_proj,
    query_gain,
    key_gain,
    norm_gain,
    routes,
    route_weight,
    expert_gate,
    expert_up,
    expert_down,
    shared_gate,
    shared_up,
    shared_down,
):
    return layer(
        queries,
        keys,
        values,
        query_gain.reshape(1, HD),
        key_gain.reshape(1, HD),
        norm_gain.reshape(1, 2048),
        routes.T,
        route_weight.T,
        residual,
        out_proj.reshape(64, 32, 2048),
        expert_gate,
        expert_up,
        expert_down,
        shared_gate,
        shared_up,
        shared_down,
    )


def solution(mesh):
    placed = (
        P("sp", "tp"),
        P("sp", "tp"),
        P("sp", "tp"),
        P(("sp", "tp"), None),
        P(),
        P(),
        P(),
        P(),
        P(("sp", "tp"), None),
        P(("sp", "tp"), None),
        P(("sp", "tp"), None, None),
        P(("sp", "tp"), None, None),
        P(("sp", "tp"), None, None),
        P(),
        P(),
        P(),
    )
    return jax.shard_map(
        body, mesh=mesh, in_specs=placed, out_specs=P(("sp", "tp"), None), check_vma=False
    )
```
